128 devices in a mesh: sp: 32 (over z, y, core), tp: 4 (over x).
Axes of the slice: x: 4, y: 4, z: 4, core: 2. Of those that a mesh axis runs over, the one named last changes fastest.
Arguments:
- middle_stream: bfloat16 [6144, 2048], P('sp', 'tp'), may hold values from -6 to 6
- output_gradient: bfloat16 [6144, 2048], P('sp', 'tp'), may hold values from -6 to 6
- routes: int32 [6144, 2], P('sp'), may hold values from 0 to 31, all different within a row; in each aligned block of 192 rows (0 to 191, 192 to 383, ...) at most 18 rows name the same one
- chosen_expert_weight: float32 [6144, 2], P('sp'), may hold values from 0.2 to 1
- expert_gate_weight: bfloat16 [32, 2048, 3584], P('sp', None, 'tp'), may hold values from -0.125 to 0.125
- expert_up_weight: bfloat16 [32, 2048, 3584], P('sp', None, 'tp'), may hold values from -0.125 to 0.125
- expert_down_weight: bfloat16 [32, 3584, 2048], P('sp', 'tp'), may hold values from -0.09375 to 0.09375
- recurrent_output_weight: bfloat16 [2048, 1024], P(None, 'tp'), may hold values from -0.1875 to 0.1875
- recurrence_input: bfloat16 [6144, 1024], P('sp', 'tp'), may hold values from -8 to 8
- output_gate_logits: bfloat16 [6144, 1024], P('sp', 'tp'), may hold values from -6 to 6
- recurrence_gate_weight: bfloat16 [8, 128, 128], replicated, may hold values from -0.5 to 0.5
- input_gate_weight: bfloat16 [8, 128, 128], replicated, may hold values from -0.5 to 0.5
- channel_decay_param: float32 [1024], P('tp'), may hold values from 4 to 13
- extra_log_decay: float32 [6144, 1024], P('sp', 'tp'), may hold values from -0.7 to 0
Outputs:
- grad_gate: bfloat16 [32, 2048, 3584], P('sp', None, 'tp')
- grad_up: bfloat16 [32, 2048, 3584], P('sp', None, 'tp')
- grad_down: bfloat16 [32, 3584, 2048], P('sp', 'tp')
- grad_out_proj: float32 [2048, 1024], P('sp', 'tp')
- grad_input: float32 [6144, 1024], P('sp', 'tp')
- grad_gate_pre: float32 [6144, 1024], P('sp', 'tp')
The draws below stay inside these ranges and needn't reach their ends.
Inputs may be any that keep to these rules, and one draw needn't show every extreme that they name: `routes`: in the rows of one index of sp no expert is named more than 18 times, a bound that some block reaches in some of them; the entries of a row differ.
All inputs are finite; a program needn't handle non-finite values.
Results may differ from the reference program's by a relative error of at most 0.017.
Values may be sent and summed in bfloat16 or wider, within the bound.
No kernel may reach another device: no remote copies, remote signals or barrier semaphores. Data moves between devices by JAX's collectives and lax.ppermute only.
A program may use at most 128 MiB of HBM per device.

```python
import math
import jax
import jax.numpy as jnp
import numpy as np
from jax import lax

D = 2048
FF = 3584
BLOCKS = 8
BW = 128
TOP = 2
TOK_DEV = 192
CHANNEL_COUNT = 1024
SEQUENCE_TOKENS = 6144
EXPERTS = 32
CAP = 18
N_SP = 32
N_TP = 4


def draw_recurrence_input(key, part):
    initial_key, second_key = jax.random.split(jax.random.fold_in(key, 11))
    base_draw = jnp.clip(jax.random.normal(initial_key, (SEQUENCE_TOKENS, CHANNEL_COUNT), jnp.float32), -4.0, 4.0)
    factor = jnp.exp(jax.random.uniform(second_key, (SEQUENCE_TOKENS // TOK_DEV, 1, 1), jnp.float32, math.log(0.5), math.log(2.0)))
    scaled = (base_draw.reshape(SEQUENCE_TOKENS // TOK_DEV, TOK_DEV, CHANNEL_COUNT) * factor).reshape(SEQUENCE_TOKENS, CHANNEL_COUNT)
    return scaled.astype(jnp.bfloat16)


def draw_channel_decay_param(key, part):
    initial_key, second_key, third_key = jax.random.split(jax.random.fold_in(key, 23), 3)
    fast_share = 0.5
    fast_pick = jax.random.uniform(initial_key, (CHANNEL_COUNT,), jnp.float32) < fast_share
    fast_rate = jnp.exp(jax.random.uniform(second_key, (CHANNEL_COUNT,), jnp.float32, math.log(0.003), math.log(0.01)))
    slow_rate = jnp.exp(jax.random.uniform(third_key, (CHANNEL_COUNT,), jnp.float32, math.log(0.05), math.log(0.3))) / SEQUENCE_TOKENS
    chosen = jnp.where(fast_pick, fast_rate, slow_rate)
    return (-jnp.log(jnp.expm1(chosen))).astype(jnp.float32)


def draw_extra_log_decay(key, part):
    initial_key, second_key = jax.random.split(jax.random.fold_in(key, 37))
    spike_mask = jax.random.uniform(initial_key, (SEQUENCE_TOKENS, CHANNEL_COUNT), jnp.float32) < 4.0 / SEQUENCE_TOKENS
    loss_history = jax.random.uniform(second_key, (SEQUENCE_TOKENS, CHANNEL_COUNT), jnp.float32, math.log(0.5), math.log(0.8))
    return jnp.where(spike_mask, loss_history, 0.0).astype(jnp.float32)


def strengthened(array, key, source, target, shards_of, factor):
    owner, partner = [(jnp.arange(array.shape[axis_at]) // (array.shape[axis_at] // shards_of)).reshape([-1 if axis == axis_at else 1 for axis in range(array.ndim)]) for axis_at in (source, target)]
    chosen = jax.random.permutation(key, shards_of)[partner]
    strong = (owner == chosen) | (owner == (partner + shards_of // 2) % shards_of)
    return jnp.where(strong, factor * array, array)


def steps_of(key, shape, cuts, smallest, top_value):
    loudness = 1.0
    for axis_at, shards_of in cuts:
        draws = jax.random.uniform(jax.random.fold_in(jax.random.fold_in(key, 6), axis_at), (shards_of,), jnp.float32, smallest / len(cuts), top_value / len(cuts))
        loudness = loudness * jnp.repeat(jnp.exp(draws), shape[axis_at] // shards_of).reshape((-1,) + (1,) * (len(shape) - 1 - axis_at))
    return loudness


def shared_out(key, own, number, rows, number_of, top, reach, skew):
    ranking = jax.random.permutation(key, number_of)
    heavy_load, ordinary = portions_of(number_of, rows * top, reach, skew, True), portions_of(number_of, rows * top, reach, skew, False)
    places = jnp.arange(number_of)

    def named(tallies, turn):
        used = int((tallies > 0).sum())
        fixed = max(1, used // 4)
        shifted = fixed + (places - fixed + turn * (used - fixed)) % max(1, number_of - fixed)
        return jnp.zeros((number_of,), jnp.int32).at[ranking[jnp.where(places < fixed, places, shifted)]].set(jnp.asarray(tallies, jnp.int32))

    tallies = jnp.where(number % 4 == 0, named(heavy_load, number // 4), named(ordinary, number - number // 4 - 1))
    mixed = jax.random.permutation(jax.random.fold_in(own, 3), number_of)
    source_of, taker = mixed[0:number_of // 2 * 2:2], mixed[1:number_of // 2 * 2:2]
    slack = jnp.minimum(tallies[source_of] - 1, reach - tallies[taker]) // 2
    slack = jnp.where((source_of == ranking[0]) | (taker == ranking[0]) | (tallies[taker] == 0), 0, jnp.maximum(slack, 0))
    shifted = jax.random.randint(jax.random.fold_in(own, 4), (number_of // 2,), 0, 1 << 20) % (slack + 1)
    tallies = tallies.at[source_of].add(-shifted).at[taker].add(shifted)
    labels = jnp.searchsorted(jnp.cumsum(tallies), jnp.arange(rows * top), side="right").astype(jnp.int32)
    listing = labels.reshape(top, rows).T
    listing = listing[jax.random.permutation(jax.random.fold_in(own, 1), rows)]
    turn = jax.random.randint(jax.random.fold_in(own, 2), (rows, 1), 0, top)
    return jnp.take_along_axis(listing, (jnp.arange(top)[None, :] + turn) % top, axis=1)


def portions_of(amount, total, bound, slope, full):
    portions = [(1 << 20) // math.isqrt(grade ** slope) + 1 for grade in range(1, amount + 1)]
    largest = bound if full else min(bound, max(-(-total // amount), total * portions[0] // sum(portions)))
    least = 1 if total - largest >= amount - 1 else 0
    holding, spare = [largest] + [least] * (amount - 1), total - largest - least * (amount - 1)
    while spare > 0:
        candidates = [i for i in range(1, amount) if holding[i] < largest] or [i for i in range(1, amount) if holding[i] < bound]
        whole, budget = sum([portions[i] for i in candidates]), spare
        for i in candidates:
            more = min(bound - holding[i], max(1, budget * portions[i] // whole), spare)
            holding[i] = holding[i] + more
            spare = spare - more
    return np.array(holding)


def bell_draw(stream_key, dims, width, bound, cuts=(), kind=jnp.bfloat16):
    array = jax.random.normal(stream_key, dims, jnp.float32) * width
    if len(cuts) > 0:
        array = steps_of(stream_key, dims, cuts, -0.22, 0.18) * array
    return jnp.clip(array, min=-bound, max=bound).astype(kind)


def noise_with(rng, dims, width, most, cuts, heavy, kind=jnp.bfloat16):
    array = width * jax.random.normal(rng, dims, jnp.float32)
    if cuts:
        array = array * steps_of(rng, dims, cuts, -0.22, 0.18)
    return jnp.clip(strengthened(array, jax.random.fold_in(rng, 3), *heavy), -most, most).astype(kind)


def setup_inputs(seed: int = 0) -> dict:
    streams_of = jax.random.split(jax.random.key(seed), 15)
    middle_stream = bell_draw(streams_of[0], (SEQUENCE_TOKENS, D), 1.0, 6.0, ((0, 32), (1, 4)))
    output_gradient = noise_with(streams_of[1], (SEQUENCE_TOKENS, D), 1.0, 6.0, ((0, 32), (1, 4)), (0, 1, 32, 2.75))
    routes_keys = jax.random.split(jax.random.fold_in(streams_of[2], 1), SEQUENCE_TOKENS // TOK_DEV)
    routes_turns = jax.random.permutation(jax.random.fold_in(streams_of[2], 3), SEQUENCE_TOKENS // TOK_DEV)
    routes = jax.vmap(lambda own, number: shared_out(jax.random.fold_in(streams_of[2], 2), own, number, TOK_DEV, EXPERTS, TOP, CAP, 1))(routes_keys, routes_turns).reshape((SEQUENCE_TOKENS, TOP))
    chosen_expert_weight = jnp.clip(0.2 + 0.8 * jax.random.uniform(streams_of[3], (SEQUENCE_TOKENS, TOP), jnp.float32) ** steps_of(streams_of[3], (SEQUENCE_TOKENS, TOP), ((0, 32),), -0.2, 0.2), 0.2, 1.0)
    expert_gate_weight = bell_draw(streams_of[4], (EXPERTS, D, FF), D ** -0.5, 0.125, ((0, 32), (2, 4)))
    expert_up_weight = bell_draw(streams_of[5], (EXPERTS, D, FF), D ** -0.5, 0.125, ((0, 32), (2, 4)))
    expert_down_weight = bell_draw(streams_of[6], (EXPERTS, FF, D), FF ** -0.5, 0.09375, ((0, 32), (1, 4)))
    recurrent_output_weight = bell_draw(streams_of[7], (D, CHANNEL_COUNT), CHANNEL_COUNT ** -0.5, 0.1875, ((1, 4),))
    recurrence_input = draw_recurrence_input(jax.random.fold_in(streams_of[14], 71), 0)
    output_gate_logits = bell_draw(streams_of[9], (SEQUENCE_TOKENS, CHANNEL_COUNT), 1.0, 6.0, ((0, 32), (1, 4)))
    recurrence_gate_weight = bell_draw(streams_of[10], (BLOCKS, BW, BW), BW ** -0.5, 0.5)
    input_gate_weight = bell_draw(streams_of[11], (BLOCKS, BW, BW), BW ** -0.5, 0.5)
    channel_decay_param = draw_channel_decay_param(jax.random.fold_in(streams_of[14], 71), 0)
    extra_log_decay = draw_extra_log_decay(jax.random.fold_in(streams_of[14], 71), 0)
    return {"middle_stream": middle_stream, "output_gradient": output_gradient, "routes": routes, "chosen_expert_weight": chosen_expert_weight, "expert_gate_weight": expert_gate_weight, "expert_up_weight": expert_up_weight, "expert_down_weight": expert_down_weight, "recurrent_output_weight": recurrent_output_weight, "recurrence_input": recurrence_input, "output_gate_logits": output_gate_logits, "recurrence_gate_weight": recurrence_gate_weight, "input_gate_weight": input_gate_weight, "channel_decay_param": channel_decay_param, "extra_log_decay": extra_log_decay}


def combine_linear(earlier, latter):
    return (earlier[0] * latter[0], latter[0] * earlier[1] + latter[1])

def linear_scan(factor, driven):
    return lax.associative_scan(combine_linear, (factor, driven), axis=0)

def gelu_parts(output_gate_logits):
    gate_float = output_gate_logits.astype(jnp.float32)
    return jax.jvp(jax.nn.gelu, (gate_float,), (jnp.ones_like(gate_float),))

def expert_backward(inputs, cotangent, gate_weight, up_weight, down_weight):
    gate_act = jnp.dot(inputs, gate_weight, preferred_element_type=jnp.float32)
    up_act = jnp.dot(inputs, up_weight, preferred_element_type=jnp.float32)
    sigmoid_gate = jax.nn.sigmoid(gate_act)
    silu_act = gate_act * sigmoid_gate
    hidden = (silu_act * up_act).astype(jnp.bfloat16)
    d_hidden = lax.dot_general(cotangent, down_weight, (((1,), (1,)), ((), ())), preferred_element_type=jnp.float32)
    grad_down = lax.dot_general(hidden, cotangent, (((0,), (0,)), ((), ())), preferred_element_type=jnp.float32)
    d_gate = (d_hidden * up_act * sigmoid_gate * (1.0 + gate_act * (1.0 - sigmoid_gate))).astype(jnp.bfloat16)
    d_up = (d_hidden * silu_act).astype(jnp.bfloat16)
    grad_gate = lax.dot_general(inputs, d_gate, (((0,), (0,)), ((), ())), preferred_element_type=jnp.float32)
    grad_up = lax.dot_general(inputs, d_up, (((0,), (0,)), ((), ())), preferred_element_type=jnp.float32)
    return (grad_gate.astype(jnp.bfloat16), grad_up.astype(jnp.bfloat16), grad_down.astype(jnp.bfloat16), d_gate, d_up)

def reference(middle_stream, output_gradient, routes, chosen_expert_weight, expert_gate_weight, expert_up_weight, expert_down_weight, recurrent_output_weight, recurrence_input, output_gate_logits, recurrence_gate_weight, input_gate_weight, channel_decay_param, extra_log_decay):
    tokens, model_width = middle_stream.shape
    top_count = routes.shape[1]
    routed = routes.reshape(-1)
    onehot = (routed[:, None] == jnp.arange(EXPERTS, dtype=jnp.int32)[None, :]).astype(jnp.int32)
    onehot = onehot.reshape(N_SP, TOK_DEV * top_count, EXPERTS)
    slot_rank = (lax.optimization_barrier(jnp.sum(jnp.cumsum(onehot, axis=1) * onehot, axis=2)) - 1).reshape(-1)
    source = jnp.arange(tokens * top_count, dtype=jnp.int32) // (TOK_DEV * top_count)
    buffer_place = (source * CAP + slot_rank).astype(jnp.int32)
    slot_table = jnp.full((EXPERTS, N_SP * CAP), tokens * top_count, jnp.int32)
    slot_table = slot_table.at[routed, buffer_place].set(jnp.arange(tokens * top_count, dtype=jnp.int32))
    zero_row = jnp.zeros((1, model_width), jnp.bfloat16)
    pair_rows = jnp.broadcast_to(middle_stream[:, None, :], (tokens, top_count, model_width)).reshape(-1, model_width)
    pair_rows = jnp.concatenate([pair_rows, zero_row], axis=0)
    pair_cot = (chosen_expert_weight[:, :, None] * output_gradient.astype(jnp.float32)[:, None, :]).astype(jnp.bfloat16)
    pair_cot = jnp.concatenate([pair_cot.reshape(-1, model_width), zero_row], axis=0)

    def one_expert(packed):
        table_row, gate_weight, up_weight, down_weight = packed
        inputs = pair_rows[table_row]
        cotangent = pair_cot[table_row]
        grad_gate, grad_up, grad_down, d_gate, d_up = expert_backward(inputs, cotangent, gate_weight, up_weight, down_weight)
        slot_rows = inputs.shape[0]
        quarter = gate_weight.shape[1] // N_TP
        gate_q = d_gate.astype(jnp.float32).reshape(slot_rows, N_TP, quarter)
        up_q = d_up.astype(jnp.float32).reshape(slot_rows, N_TP, quarter)
        gate_wq = gate_weight.astype(jnp.float32).reshape(model_width, N_TP, quarter)
        up_wq = up_weight.astype(jnp.float32).reshape(model_width, N_TP, quarter)
        partial_value = jnp.einsum('rqf,dqf->qrd', gate_q, gate_wq) + jnp.einsum('rqf,dqf->qrd', up_q, up_wq)
        rounded = lax.optimization_barrier(partial_value.astype(jnp.bfloat16)).astype(jnp.float32)
        slot_grad = lax.optimization_barrier(jnp.sum(rounded, axis=0)).astype(jnp.bfloat16)
        return (grad_gate, grad_up, grad_down, slot_grad)
    grad_gate, grad_up, grad_down, slot_grad = lax.map(one_expert, (slot_table, expert_gate_weight, expert_up_weight, expert_down_weight))
    slot_back = jnp.zeros((tokens * top_count + 1, model_width), jnp.bfloat16)
    slot_back = slot_back.at[slot_table.reshape(-1)].set(slot_grad.reshape(-1, model_width))
    arrived = slot_back[:-1].astype(jnp.float32).reshape(tokens, top_count, model_width)
    residual_grad = (output_gradient.astype(jnp.float32) + lax.optimization_barrier(jnp.sum(arrived, axis=1))).astype(jnp.bfloat16)
    mixer_grad = jnp.dot(residual_grad, recurrent_output_weight, preferred_element_type=jnp.float32)
    channels = recurrence_input.shape[1]
    blocks, block_width = (recurrence_gate_weight.shape[0], recurrence_gate_weight.shape[1])
    u_float = recurrence_input.astype(jnp.float32)
    u_blocks = u_float.reshape(tokens, blocks, block_width)
    forget_gate = jax.nn.sigmoid(jnp.einsum('tnb,nbc->tnc', u_blocks, recurrence_gate_weight.astype(jnp.float32)).reshape(tokens, channels))
    admit_gate = jax.nn.sigmoid(jnp.einsum('tnb,nbc->tnc', u_blocks, input_gate_weight.astype(jnp.float32)).reshape(tokens, channels))
    baseline_rate = jax.nn.softplus(-channel_decay_param)
    decay_logarithm = -8.0 * forget_gate * baseline_rate[None, :] + extra_log_decay
    decay_step = jnp.exp(decay_logarithm)
    input_scale = jnp.sqrt(-jnp.expm1(2.0 * decay_logarithm))
    driven = u_float * admit_gate * input_scale
    _, states = linear_scan(decay_step, driven)
    prev_states = jnp.concatenate([jnp.zeros((1, channels), jnp.float32), states[:-1]], axis=0)
    gelu_val, gelu_der = gelu_parts(output_gate_logits)
    lru_out = (states * gelu_val).astype(jnp.bfloat16)
    grad_out_proj = lax.dot_general(residual_grad, lru_out, (((0,), (0,)), ((), ())), preferred_element_type=jnp.float32)
    grad_gate_pre = mixer_grad * states * gelu_der
    state_in = mixer_grad * gelu_val
    next_decay = jnp.concatenate([decay_step[1:], jnp.zeros((1, channels), jnp.float32)], axis=0)
    _, flipped = linear_scan(next_decay[::-1], state_in[::-1])
    state_grad = flipped[::-1]
    d_log = state_grad * (prev_states * decay_step - u_float * admit_gate * decay_step * decay_step / input_scale)
    d_recall = (d_log * (-8.0 * baseline_rate[None, :]) * forget_gate * (1.0 - forget_gate)).astype(jnp.bfloat16)
    d_admit = (state_grad * u_float * input_scale * admit_gate * (1.0 - admit_gate)).astype(jnp.bfloat16)
    back_recall = jnp.einsum('tnc,nbc->tnb', d_recall.astype(jnp.float32).reshape(tokens, blocks, block_width), recurrence_gate_weight.astype(jnp.float32))
    back_admit = jnp.einsum('tnc,nbc->tnb', d_admit.astype(jnp.float32).reshape(tokens, blocks, block_width), input_gate_weight.astype(jnp.float32))
    grad_input = state_grad * admit_gate * input_scale + (back_recall + back_admit).reshape(tokens, channels)
    return (grad_gate, grad_up, grad_down, grad_out_proj, grad_input, grad_gate_pre)
```

```python
import jax
import jax.numpy as jnp
from jax import lax
from jax.experimental import pallas as pl
from jax.experimental.pallas import tpu as pltpu
from jax.sharding import PartitionSpec as P

BF = jnp.bfloat16
F32 = jnp.float32
ROWS = 192
PEERS = 32
TPN = 4
LANE = 128
CH = 256
HID = 896
WIDTH = 2048
VMEM = pl.BlockSpec(memory_space=pltpu.VMEM)
SMEM = pl.BlockSpec(memory_space=pltpu.SMEM)


def mm(a, b, ca=1, cb=0):
    return lax.dot_general(a, b, (((ca,), (cb,)), ((), ())), preferred_element_type=F32)


def iota(shape, dim):
    return lax.broadcasted_iota(jnp.int32, shape, dim)


def call(body, out, n_in, flops, moved, smem=()):
    return pl.pallas_call(
        body,
        out_shape=out,
        in_specs=[SMEM if k in smem else VMEM for k in range(n_in)],
        out_specs=jax.tree.map(lambda _: VMEM, out),
        cost_estimate=pl.CostEstimate(flops=flops, bytes_accessed=moved, transcendentals=0),
        compiler_params=pltpu.CompilerParams(vmem_limit_bytes=56 * 1024 * 1024),
    )


def pack_main(block, out, base, pieces):
    rows = block.reshape(PEERS, 8, pieces * LANE)
    for pair in range(pieces // 2):
        lo = rows[:, :, 2 * pair * LANE : (2 * pair + 1) * LANE]
        hi = rows[:, :, (2 * pair + 1) * LANE : (2 * pair + 2) * LANE]
        at = base + pair * 16
        out[:, at : at + 16, :] = jnp.concatenate([lo, hi], axis=1).astype(BF)


def unpack_main(block, pair):
    got = block[:, pair * 16 : pair * 16 + 16, :].astype(F32)
    lo = got[:, :8, :].reshape(PEERS * 8, LANE).astype(BF)
    hi = got[:, 8:, :].reshape(PEERS * 8, LANE).astype(BF)
    return lo, hi


def tail_order(pieces):
    n = PEERS * pieces * 2
    r, c = iota((n, n), 0), iota((n, n), 1)
    peer, piece, slot = r // (pieces * 2), (r // 2) % pieces, r % 2
    return (piece * (PEERS * 2) + peer * 2 + slot == c).astype(F32).astype(BF)


def tail_order_back(pieces):
    n = PEERS * pieces * 2
    r, c = iota((n, n), 0), iota((n, n), 1)
    peer, piece, slot = c // (pieces * 2), (c // 2) % pieces, c % 2
    return (piece * (PEERS * 2) + peer * 2 + slot == r).astype(F32).astype(BF)


def pack_body(routes, weights, x, g, out_a, out_b, out_idx):
    experts = iota((PEERS, ROWS), 0)
    before = (iota((ROWS, ROWS), 0) < iota((ROWS, ROWS), 1)).astype(F32).astype(BF)
    same = iota((ROWS, ROWS), 0) == iota((ROWS, ROWS), 1)
    r0, r1 = routes[0:1, :], routes[1:2, :]
    o0 = (experts == r0).astype(F32)
    o1 = (experts == r1).astype(F32)
    c0 = mm(o0.astype(BF), before)
    c1 = mm(o1.astype(BF), before) + jnp.sum(o0, axis=1, keepdims=True)
    k0 = jnp.sum(o0 * c0, axis=0, keepdims=True).astype(jnp.int32)
    k1 = jnp.sum(o1 * c1, axis=0, keepdims=True).astype(jnp.int32)
    idx = []
    for low, high in ((0, 8), (8, 16), (16, 18)):
        for r, k in ((r0, k0), (r1, k1)):
            here = (k >= low) & (k < high)
            idx.append(jnp.where(here, r * (high - low) + k - low, -1))
    none = jnp.full((1, ROWS), -1, jnp.int32)
    out_idx[...] = jnp.concatenate(idx + [none, none], axis=0)
    xv = x[...]
    gf = g[...].astype(F32)
    cots = []
    for k in range(2):
        w = jnp.sum(jnp.where(same, weights[k : k + 1, :], 0.0), axis=1, keepdims=True)
        cots.append((w * gf).astype(BF))
    both = jnp.concatenate(cots, axis=0)

    def chosen(first, n):
        r = iota((n, ROWS), 0)
        p0 = (r == idx[first]).astype(F32)
        p1 = (r == idx[first + 1]).astype(F32)
        return (
            mm((p0 + p1).astype(BF), xv),
            mm(jnp.concatenate([p0, p1], axis=1).astype(BF), both),
        )

    for first, out in ((0, out_a), (2, out_b)):
        xm, cm = chosen(first, PEERS * 8)
        pack_main(xm, out, 0, 4)
        pack_main(cm, out, 32, 4)
    xt, ct = chosen(4, PEERS * 2)
    pieces = [v[:, q * LANE : (q + 1) * LANE] for v in (xt, ct) for q in range(4)]
    tail = mm(tail_order(8), jnp.concatenate(pieces, axis=0).astype(BF))
    out_a[:, 64:80, :] = tail.astype(BF).reshape(PEERS, 16, LANE)


def chain_body(tail, tp_ref, own, left, right, far1, far2, wg, wu, wd, x, c, hid, dg, du, out):
    main = PEERS * 8
    tp = tp_ref[0]

    def at(off):
        return pl.multiple_of(((tp + off) % TPN) * 512, 512)

    if tail:
        order = tail_order_back(8)
    for off, parts in ((0, (own,)), (3, (left,)), (1, (right,)), (2, (far1, far2))):
        value = jnp.concatenate([p[...] for p in parts], axis=0) if len(parts) > 1 else parts[0][...]
        for q2 in range(4):
            lo, hi = unpack_main(value, q2)
            dest = x if q2 < 2 else c
            col = at(off) + (q2 % 2) * 256
            dest[0:main, pl.ds(col, 256)] = jnp.concatenate([lo, hi], axis=1)
        if tail:
            rows = mm(order, value[:, 64:80, :].reshape(PEERS * 16, LANE)).astype(BF)
            for q in range(8):
                dest = x if q < 4 else c
                dest[main : main + 64, pl.ds(at(off) + (q % 4) * LANE, LANE)] = rows[
                    q * 64 : (q + 1) * 64
                ]
    xv, cv = x[...], c[...]
    gate = mm(xv, wg[...])
    up = mm(xv, wu[...])
    dh = mm(cv, wd[...], 1, 1)
    sig = 1.0 / (1.0 + jnp.exp(-gate))
    silu = gate * sig
    hid[...] = (silu * up).astype(BF)
    dg[...] = (dh * up * sig * (1.0 + gate * (1.0 - sig))).astype(BF)
    du[...] = (dh * silu).astype(BF)
    dgv, duv = dg[...], du[...]
    size = 40 if tail else 32
    tails = []
    for t in range(TPN):
        part = mm(dgv, wg[t * 512 : (t + 1) * 512, :], 1, 1)
        part = part + mm(duv, wu[t * 512 : (t + 1) * 512, :], 1, 1)
        pack_main(part[:main], out, t * size, 4)
        if tail:
            pieces = [part[main:, q * LANE : (q + 1) * LANE] for q in range(4)]
            tails.append(jnp.concatenate(pieces, axis=0).astype(BF))
    if tail:
        put = mm(tail_order(4), jnp.concatenate(tails, axis=1))
        for t in range(TPN):
            out[:, t * size + 32 : t * size + 40, :] = (
                put[:, t * LANE : (t + 1) * LANE].reshape(PEERS, 8, LANE).astype(BF)
            )


def combine_body(got_a, got_b, idx, g, out):
    n = PEERS * TPN
    col = [idx[:, k : k + 1] for k in range(6)]

    def mask(code, first):
        return ((code == col[first]) | (code == col[first + 1])).astype(F32)

    m = iota((1, n * 16), 1)
    code = (m // 64) * 8 + m % 8
    half = (m // 8) % 2
    acc = [None] * 4
    for first, got in ((0, got_a), (2, got_b)):
        both = mask(code, first)
        values = [got[:, 16 * p : 16 * p + 16, :].reshape(n * 16, LANE) for p in range(2)]
        value = jnp.concatenate(values, axis=1)
        for q2 in range(2):
            r = mm(jnp.where(half == q2, both, 0.0).astype(BF), value)
            for p in range(2):
                q = 2 * p + q2
                piece = r[:, p * LANE : (p + 1) * LANE]
                acc[q] = piece if acc[q] is None else acc[q] + piece
    m = iota((1, n * 8), 1)
    both = mask((m // 32) * 2 + m % 2, 4)
    value = got_a[:, 32:40, :].reshape(n * 8, LANE)
    for q in range(4):
        acc[q] = acc[q] + mm(jnp.where((m // 2) % 4 == q, both, 0.0).astype(BF), value)
    res = (g[...].astype(F32) + jnp.concatenate(acc, axis=1)).astype(BF)
    for t in range(TPN):
        out[t] = res


def scan_body(a_ref, b_ref, cum, loc, gain, ends):
    a = a_ref[...]
    row = iota((ROWS, CH), 0)
    ca, cb = a, b_ref[...]
    step = 1
    while step < ROWS:
        ok = row >= step
        pa, pb = pltpu.roll(ca, step, 0), pltpu.roll(cb, step, 0)
        cb = jnp.where(ok, ca * pb + cb, cb)
        ca = jnp.where(ok, ca * pa, ca)
        step *= 2
    cum[...] = ca
    loc[...] = cb
    ends[0:1, :] = ca[ROWS - 1 : ROWS]
    ends[1:2, :] = cb[ROWS - 1 : ROWS]
    gn = jnp.where(row < ROWS - 1, pltpu.roll(a, ROWS - 1, 0), 1.0)
    step = 1
    while step < ROWS:
        ok = row < ROWS - step
        gn = jnp.where(ok, gn * pltpu.roll(gn, ROWS - step, 0), gn)
        step *= 2
    gain[...] = gn


def states_body(sp_ref, gains, terms, a, cum, loc, logits, q, rr, s1, gv, lru, r_out, coef):
    sp = sp_ref[0]
    row = iota((PEERS, CH), 0)
    gn = gains[...]
    fwd = jnp.where(row < sp, gn, 1.0)
    fwd = jnp.where(row < PEERS - 1, pltpu.roll(fwd, PEERS - 1, 0), 1.0)
    rev = jnp.where(row > sp, gn, 1.0)
    rev = jnp.where(row > 0, pltpu.roll(rev, 1, 0), 1.0)
    step = 1
    while step < PEERS:
        fwd = jnp.where(row < PEERS - step, fwd * pltpu.roll(fwd, PEERS - step, 0), fwd)
        rev = jnp.where(row >= step, rev * pltpu.roll(rev, step, 0), rev)
        step *= 2
    carry = jnp.sum(jnp.where(row < sp, terms[...] * fwd, 0.0), axis=0, keepdims=True)
    coef[...] = jnp.where(row > sp, rev, 0.0)
    st = loc[...] + cum[...] * carry
    wide = iota((ROWS, CH), 0)
    prev = jnp.where(wide > 0, pltpu.roll(st, 1, 0), carry)
    z = logits[...].astype(F32)
    k = 0.7978845608028654
    t = jnp.tanh(k * (z + 0.044715 * z * z * z))
    val = 0.5 * z * (1.0 + t)
    der = 0.5 * (1.0 + t) + 0.5 * z * (1.0 - t * t) * k * (1.0 + 3.0 * 0.044715 * z * z)
    s1[...] = st * der
    gv[...] = val
    lru[...] = (st * val).astype(BF)
    r_out[...] = rr[...] * (prev * a[...] - q[...])


def reverse_body(full, wout, gv, s1, lru, a_ref, gate_pre, tail_sum, send):
    mixer = mm(full[0], wout[0:512, :])
    for t in range(1, TPN):
        mixer = mixer + mm(full[t], wout[t * 512 : (t + 1) * 512, :])
    gate_pre[...] = mixer * s1[...]
    row = iota((ROWS, CH), 0)
    a = a_ref[...]
    gn = jnp.where(row < ROWS - 1, pltpu.roll(a, ROWS - 1, 0), 1.0)
    s = mixer * gv[...]
    step = 1
    while step < ROWS:
        ok = row < ROWS - step
        s = jnp.where(ok, s + gn * pltpu.roll(s, ROWS - step, 0), s)
        gn = jnp.where(ok, gn * pltpu.roll(gn, ROWS - step, 0), gn)
        step *= 2
    tail_sum[...] = s
    term = a[0:1] * s[0:1]
    hi = term.astype(BF)
    rest = term - hi.astype(F32)
    mid = rest.astype(BF)
    low = (rest - mid.astype(F32)).astype(BF)
    which = iota((8, CH), 0)
    extra = jnp.where(which == 0, hi.astype(F32), 0.0)
    extra = jnp.where(which == 1, mid.astype(F32), extra)
    extra = jnp.where(which == 2, low.astype(F32), extra).astype(BF)
    send[:, 64:72, :] = jnp.broadcast_to(extra[None], (PEERS, 8, CH))
    lv = lru[...]
    for t in range(TPN):
        part = mm(full[t], lv, 0, 0).astype(BF)
        send[8 * t : 8 * t + 8, 0:64, :] = part.reshape(8, 64, CH)


def final_body(got, coef, tail_sum, gain, rr, ad, scaled, wr, wi, out_proj, grad_in):
    acc = got[0, 0:64, :].astype(F32)
    for s in range(1, PEERS):
        acc = acc + got[s, 0:64, :].astype(F32)
    out_proj[...] = acc
    terms = jnp.sum(got[:, 64:72, :].astype(F32), axis=1)
    carry = jnp.sum(terms * coef[...], axis=0, keepdims=True)
    sg = tail_sum[...] + gain[...] * carry
    d_recall = (sg * rr[...]).astype(BF)
    d_admit = (sg * ad[...]).astype(BF)
    base = sg * scaled[...]
    for n in range(2):
        cols = slice(n * LANE, (n + 1) * LANE)
        back = mm(d_recall[:, cols], wr[n], 1, 1) + mm(d_admit[:, cols], wi[n], 1, 1)
        grad_in[:, cols] = base[:, cols] + back


RING = [(i, (i + 1) % TPN) for i in range(TPN)]
BACK = [(i, (i - 1) % TPN) for i in range(TPN)]


def ring_parts(own):
    left = lax.ppermute(own, "tp", RING)
    right = lax.ppermute(own, "tp", BACK)
    half = PEERS // 2
    far1 = lax.ppermute(left[:half], "tp", RING)
    far2 = lax.ppermute(right[half:], "tp", BACK)
    return own, left, right, far1, far2


def shape(*dims, dtype=BF):
    return jax.ShapeDtypeStruct(dims, dtype)


def expert_chain(tail, tp, parts, weights):
    rows = PEERS * (10 if tail else 8)
    size = 40 if tail else 32
    out = [shape(rows, WIDTH), shape(rows, WIDTH)] + [shape(rows, HID)] * 3
    out.append(shape(PEERS, TPN * size, LANE))

    def body(*refs):
        chain_body(tail, *refs)

    flops = 10 * rows * WIDTH * HID
    *saved, partial_value = call(body, out, 9, flops, 12 << 20, smem=(0,))(tp, *parts, *weights)
    return saved, partial_value.reshape(PEERS * TPN, size, LANE)


def per_device(
    middle_stream,
    output_gradient,
    routes,
    chosen_expert_weight,
    expert_gate_weight,
    expert_up_weight,
    expert_down_weight,
    recurrent_output_weight,
    recurrence_input,
    output_gate_logits,
    recurrence_gate_weight,
    input_gate_weight,
    channel_decay_param,
    extra_log_decay,
):
    tp = lax.axis_index("tp").reshape(1).astype(jnp.int32)
    sp = lax.axis_index("sp").reshape(1).astype(jnp.int32)
    weights = (expert_gate_weight[0], expert_up_weight[0], expert_down_weight[0])

    send_a, send_b, idx = call(
        pack_body,
        [shape(PEERS, 80, LANE), shape(PEERS, 64, LANE), shape(8, ROWS, dtype=jnp.int32)],
        4,
        1 << 30,
        3 << 20,
    )(routes.T, chosen_expert_weight.T, middle_stream, output_gradient)
    own_a = lax.all_to_all(send_a, "sp", 0, 0, tiled=True)
    own_a, send_b = lax.optimization_barrier((own_a, send_b))
    own_b = lax.all_to_all(send_b, "sp", 0, 0, tiled=True)
    parts_a = ring_parts(own_a)
    parts_b = ring_parts(own_b)

    first = lax.axis_index("tp") * 2
    recall_weight = lax.dynamic_slice_in_dim(recurrence_gate_weight, first, 2, 0)
    admit_weight = lax.dynamic_slice_in_dim(input_gate_weight, first, 2, 0)
    u_blocks = recurrence_input.reshape(ROWS, 2, LANE)

    def gate(weight):
        return jax.nn.sigmoid(
            jnp.einsum("tnb,nbc->tnc", u_blocks, weight, preferred_element_type=F32).reshape(
                ROWS, CH
            )
        )

    recall, admit = gate(recall_weight), gate(admit_weight)
    rate = -8.0 * jax.nn.softplus(-channel_decay_param)[None, :]
    log_decay = rate * recall + extra_log_decay
    decay = jnp.exp(log_decay)
    scale = jnp.sqrt(-jnp.expm1(2.0 * log_decay))
    u = recurrence_input.astype(F32)
    scaled = admit * scale
    driven = u * scaled
    minus = u * admit * decay * decay / scale
    of_recall = rate * recall * (1.0 - recall)
    of_admit = driven * (1.0 - admit)
    tile = shape(ROWS, CH, dtype=F32)
    cum, loc, gain, ends = call(
        scan_body, [tile, tile, tile, shape(2, CH, dtype=F32)], 2, 1 << 28, 1 << 20
    )(decay, driven)
    ends, own_b2 = lax.optimization_barrier((ends, own_b))
    all_ends = lax.all_to_all(
        jnp.broadcast_to(ends[None], (PEERS, 2, CH)), "sp", 0, 0, tiled=True
    )
    s1, gelu_val, lru, of_log, coef = call(
        states_body,
        [tile, tile, shape(ROWS, CH), tile, shape(PEERS, CH, dtype=F32)],
        9,
        1 << 28,
        2 << 20,
        smem=(0,),
    )(sp, all_ends[:, 0], all_ends[:, 1], decay, cum, loc, output_gate_logits, minus, of_recall)

    saved_a, part_a = expert_chain(True, tp, parts_a, weights)
    got_a = lax.all_to_all(part_a, ("sp", "tp"), 0, 0, tiled=True)
    saved_b, part_b = expert_chain(False, tp, parts_b, weights)
    got_b = lax.all_to_all(part_b, ("sp", "tp"), 0, 0, tiled=True)

    x, cot, hid, dg, du = (jnp.concatenate([a, b], axis=0) for a, b in zip(saved_a, saved_b))
    grad_gate = mm(x, dg, 0, 0).astype(BF)
    grad_up = mm(x, du, 0, 0).astype(BF)
    grad_down = mm(hid, cot, 0, 0).astype(BF)

    spread = call(combine_body, shape(TPN, ROWS, 512), 4, 1 << 31, 4 << 20)(
        got_a, got_b, idx.T, output_gradient
    )
    full = lax.all_to_all(spread, "tp", 0, 0, tiled=True)
    grad_gate_pre, tail_sum, send = call(
        reverse_body, [tile, tile, shape(PEERS, 72, CH)], 6, 1 << 30, 4 << 20
    )(full, recurrent_output_weight, gelu_val, s1, lru, decay)
    got = lax.all_to_all(send, "sp", 0, 0, tiled=True)
    grad_out_proj, grad_input = call(
        final_body, [shape(64, CH, dtype=F32), tile], 9, 1 << 28, 3 << 20
    )(got, coef, tail_sum, gain, of_log, of_admit, scaled, recall_weight, admit_weight)
    return (
        grad_gate[None],
        grad_up[None],
        grad_down[None],
        grad_out_proj,
        grad_input,
        grad_gate_pre,
    )


def solution(mesh):
    placed = (
        P("sp", "tp"),
        P("sp", "tp"),
        P("sp", None),
        P("sp", None),
        P("sp", None, "tp"),
        P("sp", None, "tp"),
        P("sp", "tp", None),
        P(None, "tp"),
        P("sp", "tp"),
        P("sp", "tp"),
        P(),
        P(),
        P("tp"),
        P("sp", "tp"),
    )
    return jax.shard_map(
        per_device,
        mesh=mesh,
        in_specs=placed,
        out_specs=(
            P("sp", None, "tp"),
            P("sp", None, "tp"),
            P("sp", "tp", None),
            P("sp", "tp"),
            P("sp", "tp"),
            P("sp", "tp"),
        ),
        check_vma=False,
    )
```

```python
import jax
import jax.numpy as jnp
from jax import lax
from jax.experimental import pallas as pl
from jax.experimental.pallas import tpu as pltpu
from jax.sharding import PartitionSpec as P

BF = jnp.bfloat16
F32 = jnp.float32
ROWS = 192
PEERS = 32
TPN = 4
LANE = 128
CH = 256
HID = 896
WIDTH = 2048
VMEM = pl.BlockSpec(memory_space=pltpu.VMEM)
SMEM = pl.BlockSpec(memory_space=pltpu.SMEM)
HBM = pl.BlockSpec(memory_space=pltpu.HBM)


def mm(a, b, ca=1, cb=0):
    return lax.dot_general(a, b, (((ca,), (cb,)), ((), ())), preferred_element_type=F32)


def iota(shape, dim):
    return lax.broadcasted_iota(jnp.int32, shape, dim)


def call(body, out, n_in, flops, moved, mib=56, smem=(), far=(), far_out=(), scratch=()):
    kinds = {**dict.fromkeys(smem, SMEM), **dict.fromkeys(far, HBM)}
    return pl.pallas_call(
        body,
        out_shape=out,
        in_specs=[kinds.get(k, VMEM) for k in range(n_in)],
        out_specs=[HBM if k in far_out else VMEM for k in range(len(out))],
        scratch_shapes=list(scratch),
        cost_estimate=pl.CostEstimate(flops=flops, bytes_accessed=moved, transcendentals=0),
        compiler_params=pltpu.CompilerParams(vmem_limit_bytes=mib * 1024 * 1024),
    )


def dma(count):
    return pltpu.SemaphoreType.DMA((count,))


def pack_main(block, out, base, pieces):
    rows = block.reshape(PEERS, 8, pieces * LANE)
    for pair in range(pieces // 2):
        lo = rows[:, :, 2 * pair * LANE : (2 * pair + 1) * LANE]
        hi = rows[:, :, (2 * pair + 1) * LANE : (2 * pair + 2) * LANE]
        at = base + pair * 16
        out[:, at : at + 16, :] = jnp.concatenate([lo, hi], axis=1).astype(BF)


def unpack_main(block, pair):
    got = block[:, pair * 16 : pair * 16 + 16, :].astype(F32)
    lo = got[:, :8, :].reshape(PEERS * 8, LANE).astype(BF)
    hi = got[:, 8:, :].reshape(PEERS * 8, LANE).astype(BF)
    return lo, hi


def tail_order(pieces):
    n = PEERS * pieces * 2
    r, c = iota((n, n), 0), iota((n, n), 1)
    peer, piece, slot = r // (pieces * 2), (r // 2) % pieces, r % 2
    return (piece * (PEERS * 2) + peer * 2 + slot == c).astype(F32).astype(BF)


def tail_order_back(pieces):
    n = PEERS * pieces * 2
    r, c = iota((n, n), 0), iota((n, n), 1)
    peer, piece, slot = c // (pieces * 2), (c // 2) % pieces, c % 2
    return (piece * (PEERS * 2) + peer * 2 + slot == r).astype(F32).astype(BF)


def pack_body(routes, weights, x, g, out_a, out_b, out_idx):
    experts = iota((PEERS, ROWS), 0)
    before = (iota((ROWS, ROWS), 0) < iota((ROWS, ROWS), 1)).astype(F32).astype(BF)
    same = iota((ROWS, ROWS), 0) == iota((ROWS, ROWS), 1)
    r0, r1 = routes[0:1, :], routes[1:2, :]
    o0 = (experts == r0).astype(F32)
    o1 = (experts == r1).astype(F32)
    c0 = mm(o0.astype(BF), before)
    c1 = mm(o1.astype(BF), before) + jnp.sum(o0, axis=1, keepdims=True)
    k0 = jnp.sum(o0 * c0, axis=0, keepdims=True).astype(jnp.int32)
    k1 = jnp.sum(o1 * c1, axis=0, keepdims=True).astype(jnp.int32)
    idx = []
    for low, high in ((0, 8), (8, 16), (16, 18)):
        for r, k in ((r0, k0), (r1, k1)):
            here = (k >= low) & (k < high)
            idx.append(jnp.where(here, r * (high - low) + k - low, -1))
    none = jnp.full((1, ROWS), -1, jnp.int32)
    out_idx[...] = jnp.concatenate(idx + [none, none], axis=0)
    xv = x[...]
    gf = g[...].astype(F32)
    cots = []
    for k in range(2):
        w = jnp.sum(jnp.where(same, weights[k : k + 1, :], 0.0), axis=1, keepdims=True)
        cots.append((w * gf).astype(BF))
    both = jnp.concatenate(cots, axis=0)

    def chosen(first, n):
        r = iota((n, ROWS), 0)
        p0 = (r == idx[first]).astype(F32)
        p1 = (r == idx[first + 1]).astype(F32)
        return (
            mm((p0 + p1).astype(BF), xv),
            mm(jnp.concatenate([p0, p1], axis=1).astype(BF), both),
        )

    for first, out in ((0, out_a), (2, out_b)):
        xm, cm = chosen(first, PEERS * 8)
        pack_main(xm, out, 0, 4)
        pack_main(cm, out, 32, 4)
    xt, ct = chosen(4, PEERS * 2)
    pieces = [v[:, q * LANE : (q + 1) * LANE] for v in (xt, ct) for q in range(4)]
    tail = mm(tail_order(8), jnp.concatenate(pieces, axis=0).astype(BF))
    out_a[:, 64:80, :] = tail.astype(BF).reshape(PEERS, 16, LANE)


def chain_body(tail, tp_ref, *refs):
    parts, weights, outs, rest = refs[:7], refs[7:10], refs[10:16], refs[16:]
    values, x, c, hid, dg, du, out, wg, wu, wd, sem_in, sem_w, sem_out = rest
    main = PEERS * 8
    half = PEERS // 2
    depth = 80 if tail else 64
    size = 40 if tail else 32
    places = [values.at[0]] + [values.at[s, pl.ds(h * half, half)] for s in (1, 2, 3) for h in (0, 1)]
    fetch = [
        pltpu.make_async_copy(p.at[:, 0:depth] if k == 0 else p, place, sem_in.at[k])
        for k, (p, place) in enumerate(zip(parts, places))
    ]
    loads = [
        pltpu.make_async_copy(w, v, sem_w.at[k])
        for k, (w, v) in enumerate(zip(weights, (wg, wu, wd)))
    ]
    for copy in fetch + loads:
        copy.start()
    saves = [
        pltpu.make_async_copy(v, o, sem_out.at[k])
        for k, (v, o) in enumerate(zip((x, c, hid, dg, du), outs))
    ]
    saves += [
        pltpu.make_async_copy(
            out.at[:, t * size : (t + 1) * size], outs[5].at[:, t * size : (t + 1) * size], sem_out.at[5 + t]
        )
        for t in range(TPN)
    ]
    tp = tp_ref[0]

    def at(off):
        return pl.multiple_of(((tp + off) % TPN) * 512, 512)

    if tail:
        order = tail_order_back(8)
    for source, (off, arriving) in enumerate(((0, (0,)), (3, (1, 2)), (1, (3, 4)), (2, (5, 6)))):
        for k in arriving:
            fetch[k].wait()
        value = values[source]
        for q2 in range(4):
            lo, hi = unpack_main(value, q2)
            dest = x if q2 < 2 else c
            col = at(off) + (q2 % 2) * 256
            dest[0:main, pl.ds(col, 256)] = jnp.concatenate([lo, hi], axis=1)
        if tail:
            rows = mm(order, value[:, 64:80, :].reshape(PEERS * 16, LANE)).astype(BF)
            for q in range(8):
                dest = x if q < 4 else c
                dest[main : main + 64, pl.ds(at(off) + (q % 4) * LANE, LANE)] = rows[
                    q * 64 : (q + 1) * 64
                ]
    saves[0].start()
    saves[1].start()
    xv, cv = x[...], c[...]
    loads[0].wait()
    gate = mm(xv, wg[...])
    loads[1].wait()
    up = mm(xv, wu[...])
    loads[2].wait()
    dh = mm(cv, wd[...], 1, 1)
    sig = 1.0 / (1.0 + jnp.exp(-gate))
    silu = gate * sig
    hid[...] = (silu * up).astype(BF)
    dg[...] = (dh * up * sig * (1.0 + gate * (1.0 - sig))).astype(BF)
    du[...] = (dh * silu).astype(BF)
    for k in (2, 3, 4):
        saves[k].start()
    dgv, duv = dg[...], du[...]
    if tail:
        order = tail_order(4)
    for t in range(TPN):
        part = mm(dgv, wg[t * 512 : (t + 1) * 512, :], 1, 1)
        part = part + mm(duv, wu[t * 512 : (t + 1) * 512, :], 1, 1)
        pack_main(part[:main], out, t * size, 4)
        if tail:
            pieces = [part[main:, q * LANE : (q + 1) * LANE] for q in range(4)]
            put = mm(order, jnp.concatenate(pieces, axis=0).astype(BF))
            out[:, t * size + 32 : t * size + 40, :] = put.reshape(PEERS, 8, LANE).astype(BF)
        saves[5 + t].start()
    for save in saves:
        save.wait()


def slot_mask(idx, code, first):
    at0, at1 = idx[:, first : first + 1], idx[:, first + 1 : first + 2]
    return ((code == at0) | (code == at1)).astype(F32)


def add_main(got, idx, first):
    n = PEERS * TPN
    m = iota((1, n * 16), 1)
    both = slot_mask(idx, (m // 64) * 8 + m % 8, first)
    half = (m // 8) % 2
    values = [got[:, 16 * p : 16 * p + 16, :].reshape(n * 16, LANE) for p in range(2)]
    value = jnp.concatenate(values, axis=1)
    even, odd = [mm(jnp.where(half == k, both, 0.0).astype(BF), value) for k in range(2)]
    return [even[:, :LANE], odd[:, :LANE], even[:, LANE:], odd[:, LANE:]]


def combine_a_body(got, idx, g, out):
    n = PEERS * TPN
    acc = add_main(got, idx, 0)
    m = iota((1, n * 8), 1)
    both = slot_mask(idx, (m // 32) * 2 + m % 2, 4)
    value = got[:, 32:40, :].reshape(n * 8, LANE)
    for q in range(4):
        acc[q] = acc[q] + mm(jnp.where((m // 2) % 4 == q, both, 0.0).astype(BF), value)
    out[...] = g[...].astype(F32) + jnp.concatenate(acc, axis=1)


def combine_b_body(got, idx, so_far, out, res, sem):
    acc = add_main(got, idx, 2)
    res[...] = (so_far[...] + jnp.concatenate(acc, axis=1)).astype(BF)
    copies = [pltpu.make_async_copy(res, out.at[t], sem.at[t]) for t in range(TPN)]
    for copy in copies:
        copy.start()
    for copy in copies:
        copy.wait()


def in_three(v):
    hi = v.astype(BF)
    rest = v - hi.astype(F32)
    mid = rest.astype(BF)
    low = (rest - mid.astype(F32)).astype(BF)
    return [p.astype(F32) for p in (hi, mid, low)]


def scan_body(a_ref, b_ref, rows_b, cum, loc, gain, send):
    a = a_ref[...]
    row = iota((ROWS, CH), 0)
    ca, cb = a, b_ref[...]
    step = 1
    while step < ROWS:
        ok = row >= step
        pa, pb = pltpu.roll(ca, step, 0), pltpu.roll(cb, step, 0)
        cb = jnp.where(ok, ca * pb + cb, cb)
        ca = jnp.where(ok, ca * pa, ca)
        step *= 2
    cum[...] = ca
    loc[...] = cb
    lines = []
    for v in (ca[ROWS - 1 : ROWS], cb[ROWS - 1 : ROWS]):
        pieces = in_three(v)
        for h in range(2):
            lines += [p[:, h * LANE : (h + 1) * LANE] for p in pieces]
    lines.append(jnp.zeros((4, LANE), F32))
    extra = jnp.concatenate(lines, axis=0).astype(BF)
    send[:, 0:64, :] = rows_b[...]
    send[:, 64:80, :] = jnp.broadcast_to(extra[None], (PEERS, 16, LANE))
    gn = jnp.where(row < ROWS - 1, pltpu.roll(a, ROWS - 1, 0), 1.0)
    step = 1
    while step < ROWS:
        ok = row < ROWS - step
        gn = jnp.where(ok, gn * pltpu.roll(gn, ROWS - step, 0), gn)
        step *= 2
    gain[...] = gn


def states_body(sp_ref, got, a, cum, loc, logits, q, rr, s1, gv, lru, r_out, coef):
    sp = sp_ref[0]
    row = iota((PEERS, CH), 0)
    ends = got[:, 64:80, :].astype(F32)
    line = iota((PEERS, 16, LANE), 1)
    halves = [jnp.sum(jnp.where(line // 3 == k, ends, 0.0), axis=1) for k in range(4)]
    gn = jnp.concatenate(halves[:2], axis=1)
    terms = jnp.concatenate(halves[2:], axis=1)
    fwd = jnp.where(row < sp, gn, 1.0)
    fwd = jnp.where(row < PEERS - 1, pltpu.roll(fwd, PEERS - 1, 0), 1.0)
    rev = jnp.where(row > sp, gn, 1.0)
    rev = jnp.where(row > 0, pltpu.roll(rev, 1, 0), 1.0)
    step = 1
    while step < PEERS:
        fwd = jnp.where(row < PEERS - step, fwd * pltpu.roll(fwd, PEERS - step, 0), fwd)
        rev = jnp.where(row >= step, rev * pltpu.roll(rev, step, 0), rev)
        step *= 2
    carry = jnp.sum(jnp.where(row < sp, terms * fwd, 0.0), axis=0, keepdims=True)
    coef[...] = jnp.where(row > sp, rev, 0.0)
    st = loc[...] + cum[...] * carry
    wide = iota((ROWS, CH), 0)
    prev = jnp.where(wide > 0, pltpu.roll(st, 1, 0), carry)
    z = logits[...].astype(F32)
    k = 0.7978845608028654
    t = jnp.tanh(k * (z + 0.044715 * z * z * z))
    val = 0.5 * z * (1.0 + t)
    der = 0.5 * (1.0 + t) + 0.5 * z * (1.0 - t * t) * k * (1.0 + 3.0 * 0.044715 * z * z)
    s1[...] = st * der
    gv[...] = val
    lru[...] = (st * val).astype(BF)
    r_out[...] = rr[...] * (prev * a[...] - q[...])


def reverse_body(full, wout, gv, s1, lru, a_ref, gate_pre, tail_sum, out, send, sem):
    mixer = mm(full[0], wout[0:512, :])
    for t in range(1, TPN):
        mixer = mixer + mm(full[t], wout[t * 512 : (t + 1) * 512, :])
    gate_pre[...] = mixer * s1[...]
    row = iota((ROWS, CH), 0)
    a = a_ref[...]
    gn = jnp.where(row < ROWS - 1, pltpu.roll(a, ROWS - 1, 0), 1.0)
    s = mixer * gv[...]
    step = 1
    while step < ROWS:
        ok = row < ROWS - step
        s = jnp.where(ok, s + gn * pltpu.roll(s, ROWS - step, 0), s)
        gn = jnp.where(ok, gn * pltpu.roll(gn, ROWS - step, 0), gn)
        step *= 2
    tail_sum[...] = s
    term = a[0:1] * s[0:1]
    pieces = jnp.concatenate(in_three(term) + [jnp.zeros((5, CH), F32)], axis=0).astype(BF)
    send[:, 64:72, :] = jnp.broadcast_to(pieces[None], (PEERS, 8, CH))
    lv = lru[...]
    copies = []
    for t in range(TPN):
        part = mm(full[t], lv, 0, 0).astype(BF)
        send[8 * t : 8 * t + 8, 0:64, :] = part.reshape(8, 64, CH)
        rows = pl.ds(8 * t, 8)
        copies.append(pltpu.make_async_copy(send.at[rows], out.at[rows], sem.at[t]))
        copies[t].start()
    for copy in copies:
        copy.wait()


def final_body(got, coef, tail_sum, gain, rr, ad, scaled, wr, wi, out_proj, grad_in):
    acc = got[0, 0:64, :].astype(F32)
    for s in range(1, PEERS):
        acc = acc + got[s, 0:64, :].astype(F32)
    out_proj[...] = acc
    terms = jnp.sum(got[:, 64:72, :].astype(F32), axis=1)
    carry = jnp.sum(terms * coef[...], axis=0, keepdims=True)
    sg = tail_sum[...] + gain[...] * carry
    d_recall = (sg * rr[...]).astype(BF)
    d_admit = (sg * ad[...]).astype(BF)
    base = sg * scaled[...]
    for n in range(2):
        cols = slice(n * LANE, (n + 1) * LANE)
        back = mm(d_recall[:, cols], wr[n], 1, 1) + mm(d_admit[:, cols], wi[n], 1, 1)
        grad_in[:, cols] = base[:, cols] + back


RING = [(i, (i + 1) % TPN) for i in range(TPN)]
BACK = [(i, (i - 1) % TPN) for i in range(TPN)]


def ring_parts(own, name):
    half = PEERS // 2
    depth = own.shape[1] if name == "a" else 64
    low, high = own[:half, :depth], own[half:, :depth]

    def move(value, where):
        return lax.ppermute(value, "tp", where)

    left1 = move(low, RING)
    right2 = move(high, BACK)
    left2 = move(high, RING)
    right1 = move(low, BACK)
    far1 = move(left1, RING)
    far2 = move(right2, BACK)
    return own, left1, left2, right1, right2, far1, far2


def shape(*dims, dtype=BF):
    return jax.ShapeDtypeStruct(dims, dtype)


def expert_chain(tail, tp, parts, weights):
    rows = PEERS * (10 if tail else 8)
    size = 40 if tail else 32
    out = [shape(rows, WIDTH), shape(rows, WIDTH)] + [shape(rows, HID)] * 3
    out.append(shape(PEERS, TPN * size, LANE))

    def body(*refs):
        chain_body(tail, *refs)

    flops = 10 * rows * WIDTH * HID
    held = [(TPN, PEERS, 80 if tail else 64, LANE)] + [o.shape for o in out]
    held += [(WIDTH, HID), (WIDTH, HID), (HID, WIDTH)]
    scratch = [pltpu.VMEM(dims, BF) for dims in held] + [dma(7), dma(3), dma(9)]
    *saved, partial_value = call(
        body,
        out,
        11,
        flops,
        12 << 20,
        smem=(0,),
        far=range(1, 11),
        far_out=range(6),
        scratch=scratch,
    )(tp, *parts, *weights)
    return saved, partial_value.reshape(PEERS * TPN, size, LANE)


def per_device(
    middle_stream,
    output_gradient,
    routes,
    chosen_expert_weight,
    expert_gate_weight,
    expert_up_weight,
    expert_down_weight,
    recurrent_output_weight,
    recurrence_input,
    output_gate_logits,
    recurrence_gate_weight,
    input_gate_weight,
    channel_decay_param,
    extra_log_decay,
):
    tp = lax.axis_index("tp").reshape(1).astype(jnp.int32)
    sp = lax.axis_index("sp").reshape(1).astype(jnp.int32)
    weights = (expert_gate_weight[0], expert_up_weight[0], expert_down_weight[0])

    send_a, send_b, idx = call(
        pack_body,
        [shape(PEERS, 80, LANE), shape(PEERS, 64, LANE), shape(8, ROWS, dtype=jnp.int32)],
        4,
        1 << 30,
        3 << 20,
    )(routes.T, chosen_expert_weight.T, middle_stream, output_gradient)
    own_a = lax.all_to_all(send_a, "sp", 0, 0, tiled=True)
    first = lax.axis_index("tp") * 2
    recall_weight = lax.dynamic_slice_in_dim(recurrence_gate_weight, first, 2, 0)
    admit_weight = lax.dynamic_slice_in_dim(input_gate_weight, first, 2, 0)
    u_blocks = recurrence_input.reshape(ROWS, 2, LANE)

    def gate(weight):
        return jax.nn.sigmoid(
            jnp.einsum("tnb,nbc->tnc", u_blocks, weight, preferred_element_type=F32).reshape(
                ROWS, CH
            )
        )

    recall, admit = gate(recall_weight), gate(admit_weight)
    rate = -8.0 * jax.nn.softplus(-channel_decay_param)[None, :]
    log_decay = rate * recall + extra_log_decay
    decay = jnp.exp(log_decay)
    scale = jnp.sqrt(-jnp.expm1(2.0 * log_decay))
    u = recurrence_input.astype(F32)
    scaled = admit * scale
    driven = u * scaled
    minus = u * admit * decay * decay / scale
    of_recall = rate * recall * (1.0 - recall)
    of_admit = driven * (1.0 - admit)
    tile = shape(ROWS, CH, dtype=F32)
    cum, loc, gain, send_b = call(
        scan_body, [tile, tile, tile, shape(PEERS, 80, LANE)], 3, 1 << 28, 2 << 20
    )(decay, driven, send_b)
    own_a, send_b = lax.optimization_barrier((own_a, send_b))
    own_b = lax.all_to_all(send_b, "sp", 0, 0, tiled=True)
    parts_a = ring_parts(own_a, "a")
    parts_b = ring_parts(own_b, "b")
    s1, gelu_val, lru, of_log, coef = call(
        states_body,
        [tile, tile, shape(ROWS, CH), tile, shape(PEERS, CH, dtype=F32)],
        8,
        1 << 28,
        2 << 20,
        smem=(0,),
    )(sp, own_b, decay, cum, loc, output_gate_logits, minus, of_recall)

    saved_a, part_a = expert_chain(True, tp, parts_a, weights)
    got_a = lax.all_to_all(part_a, ("sp", "tp"), 0, 0, tiled=True)
    saved_b, part_b = expert_chain(False, tp, parts_b, weights)
    got_b = lax.all_to_all(part_b, ("sp", "tp"), 0, 0, tiled=True)

    x, cot, hid, dg, du = (jnp.concatenate([a, b], axis=0) for a, b in zip(saved_a, saved_b))
    grad_gate = mm(x, dg, 0, 0).astype(BF)
    grad_up = mm(x, du, 0, 0).astype(BF)
    grad_down = mm(hid, cot, 0, 0).astype(BF)

    columns = idx.T
    (so_far,) = call(combine_a_body, [shape(ROWS, 512, dtype=F32)], 3, 1 << 30, 2 << 20, 12)(
        got_a, columns, output_gradient
    )
    (spread,) = call(
        combine_b_body,
        [shape(TPN, ROWS, 512)],
        3,
        1 << 30,
        3 << 20,
        12,
        far_out=(0,),
        scratch=[pltpu.VMEM((ROWS, 512), BF), dma(TPN)],
    )(got_b, columns, so_far)
    full = lax.all_to_all(spread, "tp", 0, 0, tiled=True)
    grad_gate_pre, tail_sum, send = call(
        reverse_body,
        [tile, tile, shape(PEERS, 72, CH)],
        6,
        1 << 30,
        4 << 20,
        12,
        far_out=(2,),
        scratch=[pltpu.VMEM((PEERS, 72, CH), BF), dma(TPN)],
    )(full, recurrent_output_weight, gelu_val, s1, lru, decay)
    got = lax.all_to_all(send, "sp", 0, 0, tiled=True)
    grad_out_proj, grad_input = call(
        final_body, [shape(64, CH, dtype=F32), tile], 9, 1 << 28, 3 << 20, 8
    )(got, coef, tail_sum, gain, of_log, of_admit, scaled, recall_weight, admit_weight)
    return (
        grad_gate[None],
        grad_up[None],
        grad_down[None],
        grad_out_proj,
        grad_input,
        grad_gate_pre,
    )


def solution(mesh):
    placed = (
        P("sp", "tp"),
        P("sp", "tp"),
        P("sp", None),
        P("sp", None),
        P("sp", None, "tp"),
        P("sp", None, "tp"),
        P("sp", "tp", None),
        P(None, "tp"),
        P("sp", "tp"),
        P("sp", "tp"),
        P(),
        P(),
        P("tp"),
        P("sp", "tp"),
    )

    return jax.shard_map(
        per_device,
        mesh=mesh,
        in_specs=placed,
        out_specs=(
            P("sp", None, "tp"),
            P("sp", None, "tp"),
            P("sp", "tp", None),
            P("sp", "tp"),
            P("sp", "tp"),
            P("sp", "tp"),
        ),
        check_vma=False,
    )
```

```python
import jax
import jax.numpy as jnp
from jax import lax
from jax.experimental import pallas as pl
from jax.experimental.pallas import tpu as pltpu
from jax.sharding import PartitionSpec as P

BF = jnp.bfloat16
F32 = jnp.float32
ROWS = 192
PEERS = 32
TPN = 4
LANE = 128
CH = 256
HID = 896
WIDTH = 2048
VMEM = pl.BlockSpec(memory_space=pltpu.VMEM)
SMEM = pl.BlockSpec(memory_space=pltpu.SMEM)
HBM = pl.BlockSpec(memory_space=pltpu.HBM)


def mm(a, b, ca=1, cb=0):
    return lax.dot_general(a, b, (((ca,), (cb,)), ((), ())), preferred_element_type=F32)


def iota(shape, dim):
    return lax.broadcasted_iota(jnp.int32, shape, dim)


def call(body, out, n_in, flops, moved, mib=56, smem=(), far=(), far_out=(), scratch=()):
    kinds = {**dict.fromkeys(smem, SMEM), **dict.fromkeys(far, HBM)}
    return pl.pallas_call(
        body,
        out_shape=out,
        in_specs=[kinds.get(k, VMEM) for k in range(n_in)],
        out_specs=[HBM if k in far_out else VMEM for k in range(len(out))],
        scratch_shapes=list(scratch),
        cost_estimate=pl.CostEstimate(flops=flops, bytes_accessed=moved, transcendentals=0),
        compiler_params=pltpu.CompilerParams(vmem_limit_bytes=mib * 1024 * 1024),
    )


def dma(count):
    return pltpu.SemaphoreType.DMA((count,))


def pack_main(block, out, base, pieces):
    rows = block.reshape(PEERS, 8, pieces * LANE)
    for pair in range(pieces // 2):
        lo = rows[:, :, 2 * pair * LANE : (2 * pair + 1) * LANE]
        hi = rows[:, :, (2 * pair + 1) * LANE : (2 * pair + 2) * LANE]
        at = base + pair * 16
        out[:, at : at + 16, :] = jnp.concatenate([lo, hi], axis=1).astype(BF)


def unpack_main(block, pair):
    got = block[:, pair * 16 : pair * 16 + 16, :].astype(F32)
    lo = got[:, :8, :].reshape(PEERS * 8, LANE).astype(BF)
    hi = got[:, 8:, :].reshape(PEERS * 8, LANE).astype(BF)
    return lo, hi


def tail_order(pieces):
    n = PEERS * pieces * 2
    r, c = iota((n, n), 0), iota((n, n), 1)
    peer, piece, slot = r // (pieces * 2), (r // 2) % pieces, r % 2
    return (piece * (PEERS * 2) + peer * 2 + slot == c).astype(F32).astype(BF)


def tail_order_back(pieces):
    n = PEERS * pieces * 2
    r, c = iota((n, n), 0), iota((n, n), 1)
    peer, piece, slot = c // (pieces * 2), (c // 2) % pieces, c % 2
    return (piece * (PEERS * 2) + peer * 2 + slot == r).astype(F32).astype(BF)


def weighted(weights, g):
    same = iota((ROWS, ROWS), 0) == iota((ROWS, ROWS), 1)
    gf = g[...].astype(F32)
    cots = []
    for k in range(2):
        w = jnp.sum(jnp.where(same, weights[k : k + 1, :], 0.0), axis=1, keepdims=True)
        cots.append((w * gf).astype(BF))
    return jnp.concatenate(cots, axis=0)


def chosen(at0, at1, n, x, both):
    r = iota((n, ROWS), 0)
    p0, p1 = (r == at0).astype(F32), (r == at1).astype(F32)
    return (
        mm((p0 + p1).astype(BF), x),
        mm(jnp.concatenate([p0, p1], axis=1).astype(BF), both),
    )


def pack_body(routes, weights, x, g, out_a, out_idx):
    experts = iota((PEERS, ROWS), 0)
    before = (iota((ROWS, ROWS), 0) < iota((ROWS, ROWS), 1)).astype(F32).astype(BF)
    r0, r1 = routes[0:1, :], routes[1:2, :]
    o0 = (experts == r0).astype(F32)
    o1 = (experts == r1).astype(F32)
    c0 = mm(o0.astype(BF), before)
    c1 = mm(o1.astype(BF), before) + jnp.sum(o0, axis=1, keepdims=True)
    k0 = jnp.sum(o0 * c0, axis=0, keepdims=True).astype(jnp.int32)
    k1 = jnp.sum(o1 * c1, axis=0, keepdims=True).astype(jnp.int32)
    idx = []
    for low, high in ((0, 8), (8, 16), (16, 18)):
        for r, k in ((r0, k0), (r1, k1)):
            here = (k >= low) & (k < high)
            idx.append(jnp.where(here, r * (high - low) + k - low, -1))
    none = jnp.full((1, ROWS), -1, jnp.int32)
    out_idx[...] = jnp.concatenate(idx + [none, none], axis=0)
    both = weighted(weights, g)
    xv = x[...]
    xm, cm = chosen(idx[0], idx[1], PEERS * 8, xv, both)
    pack_main(xm, out_a, 0, 4)
    pack_main(cm, out_a, 32, 4)


def chain_body(tail, tp_ref, *refs):
    n = 5 if tail else 7
    parts, weights, outs, rest = refs[:n], refs[n : n + 3], refs[n + 3 : n + 9], refs[n + 9 :]
    values, x, c, hid, dg, du, out, wg, wu, wd, sem_in, sem_w, sem_out = rest
    main = PEERS * 8
    half = PEERS // 2
    depth = 80 if tail else 64
    size = 40 if tail else 32
    if tail:
        places = [values.at[0], values.at[1], values.at[2]]
        arrivals = ((0,), (1,), (2,), (3, 4))
    else:
        places = [values.at[0]] + [values.at[s, pl.ds(h * half, half)] for s in (1, 2) for h in (0, 1)]
        arrivals = ((0,), (1, 2), (3, 4), (5, 6))
    places += [values.at[3, pl.ds(h * half, half)] for h in (0, 1)]
    fetch = [
        pltpu.make_async_copy(p.at[:, 0:depth] if k == 0 else p, place, sem_in.at[k])
        for k, (p, place) in enumerate(zip(parts, places))
    ]
    loads = []
    for k, (w, v) in enumerate(zip(weights, (wg, wu, wd))):
        n = w.shape[0] // 2
        loads += [
            pltpu.make_async_copy(w.at[pl.ds(h * n, n)], v.at[pl.ds(h * n, n)], sem_w.at[2 * k + h])
            for h in range(2)
        ]
    for copy in fetch + loads[:2]:
        copy.start()
    saves = [
        pltpu.make_async_copy(v, o, sem_out.at[k])
        for k, (v, o) in enumerate(zip((x, c, hid, dg, du), outs))
    ]
    saves += [
        pltpu.make_async_copy(
            out.at[:, t * size : (t + 1) * size], outs[5].at[:, t * size : (t + 1) * size], sem_out.at[5 + t]
        )
        for t in range(TPN)
    ]
    tp = tp_ref[0]

    def at(off):
        return pl.multiple_of(((tp + off) % TPN) * 512, 512)

    if tail:
        order = tail_order_back(8)
    for source, (off, arriving) in enumerate(zip((0, 3, 1, 2), arrivals)):
        for k in arriving:
            fetch[k].wait()
        if source == 3:
            for load in loads[2:]:
                load.start()
        value = values[source]
        for q2 in range(4):
            lo, hi = unpack_main(value, q2)
            dest = x if q2 < 2 else c
            col = at(off) + (q2 % 2) * 256
            dest[0:main, pl.ds(col, 256)] = jnp.concatenate([lo, hi], axis=1)
    if tail:
        lines = [values[source, :, 64:80, :].reshape(PEERS * 16, LANE) for source in range(TPN)]
        rows = mm(order, jnp.concatenate(lines, axis=1)).astype(BF)
        for source, off in enumerate((0, 3, 1, 2)):
            cols = slice(source * LANE, (source + 1) * LANE)
            for q in range(8):
                dest = x if q < 4 else c
                dest[main : main + 64, pl.ds(at(off) + (q % 4) * LANE, LANE)] = rows[
                    q * 64 : (q + 1) * 64, cols
                ]
    xv, cv = x[...], c[...]
    for load in loads[0:2]:
        load.wait()
    gate = mm(xv, wg[...])
    for load in loads[2:4]:
        load.wait()
    up = mm(xv, wu[...])
    for load in loads[4:6]:
        load.wait()
    dh = mm(cv, wd[...], 1, 1)
    saves[0].start()
    saves[1].start()
    sig = 1.0 / (1.0 + jnp.exp(-gate))
    silu = gate * sig
    hid[...] = (silu * up).astype(BF)
    dg[...] = (dh * up * sig * (1.0 + gate * (1.0 - sig))).astype(BF)
    du[...] = (dh * silu).astype(BF)
    for k in (2, 3, 4):
        saves[k].start()
    dgv, duv = dg[...], du[...]
    if tail:
        order = tail_order(4)
    for t in range(TPN):
        part = mm(dgv, wg[t * 512 : (t + 1) * 512, :], 1, 1)
        part = part + mm(duv, wu[t * 512 : (t + 1) * 512, :], 1, 1)
        pack_main(part[:main], out, t * size, 4)
        if tail:
            pieces = [part[main:, q * LANE : (q + 1) * LANE] for q in range(4)]
            put = mm(order, jnp.concatenate(pieces, axis=0).astype(BF))
            out[:, t * size + 32 : t * size + 40, :] = put.reshape(PEERS, 8, LANE).astype(BF)
        saves[5 + t].start()
    for save in saves:
        save.wait()


def slot_mask(idx, code, first):
    at0, at1 = idx[:, first : first + 1], idx[:, first + 1 : first + 2]
    return ((code == at0) | (code == at1)).astype(F32)


def add_main(got, idx, first):
    n = PEERS * TPN
    m = iota((1, n * 16), 1)
    both = slot_mask(idx, (m // 64) * 8 + m % 8, first)
    half = (m // 8) % 2
    values = [got[:, 16 * p : 16 * p + 16, :].reshape(n * 16, LANE) for p in range(2)]
    value = jnp.concatenate(values, axis=1)
    even, odd = [mm(jnp.where(half == k, both, 0.0).astype(BF), value) for k in range(2)]
    return [even[:, :LANE], odd[:, :LANE], even[:, LANE:], odd[:, LANE:]]


def combine_a_body(got, idx, g, out):
    out[...] = g[...].astype(F32) + jnp.concatenate(add_main(got, idx, 0), axis=1)


def bring(pairs, sem):
    copies = [pltpu.make_async_copy(src, dst, sem.at[k]) for k, (src, dst) in enumerate(pairs)]
    for copy in copies:
        copy.start()
    return copies


def combine_b_body(got, idx, so_far_far, out, res, so_far, sem_in, sem):
    (early,) = bring([(so_far_far, so_far)], sem_in)
    n = PEERS * TPN
    acc = add_main(got, idx, 2)
    m = iota((1, n * 8), 1)
    both = slot_mask(idx, (m // 32) * 2 + m % 2, 4)
    value = got[:, 32:40, :].reshape(n * 8, LANE)
    for q in range(4):
        acc[q] = acc[q] + mm(jnp.where((m // 2) % 4 == q, both, 0.0).astype(BF), value)
    early.wait()
    res[...] = (so_far[...] + jnp.concatenate(acc, axis=1)).astype(BF)
    copies = [pltpu.make_async_copy(res, out.at[t], sem.at[t]) for t in range(TPN)]
    for copy in copies:
        copy.start()
    for copy in copies:
        copy.wait()


def in_three(v):
    hi = v.astype(BF)
    rest = v - hi.astype(F32)
    mid = rest.astype(BF)
    low = (rest - mid.astype(F32)).astype(BF)
    return [p.astype(F32) for p in (hi, mid, low)]


def scan_body(a_ref, b_ref, idx, weights, x, g, cum, loc, gain, send):
    both = weighted(weights, g)
    xv = x[...]
    xm, cm = chosen(idx[2:3, :], idx[3:4, :], PEERS * 8, xv, both)
    pack_main(xm, send, 0, 4)
    pack_main(cm, send, 32, 4)
    xt, ct = chosen(idx[4:5, :], idx[5:6, :], PEERS * 2, xv, both)
    pieces = [v[:, q * LANE : (q + 1) * LANE] for v in (xt, ct) for q in range(4)]
    tail = mm(tail_order(8), jnp.concatenate(pieces, axis=0).astype(BF))
    send[:, 64:80, :] = tail.astype(BF).reshape(PEERS, 16, LANE)
    a = a_ref[...]
    row = iota((ROWS, CH), 0)
    ca, cb = a, b_ref[...]
    step = 1
    while step < ROWS:
        ok = row >= step
        pa, pb = pltpu.roll(ca, step, 0), pltpu.roll(cb, step, 0)
        cb = jnp.where(ok, ca * pb + cb, cb)
        ca = jnp.where(ok, ca * pa, ca)
        step *= 2
    cum[...] = ca
    loc[...] = cb
    lines = []
    for v in (ca[ROWS - 1 : ROWS], cb[ROWS - 1 : ROWS]):
        pieces = in_three(v)
        for h in range(2):
            lines += [p[:, h * LANE : (h + 1) * LANE] for p in pieces]
    lines.append(jnp.zeros((4, LANE), F32))
    extra = jnp.concatenate(lines, axis=0).astype(BF)
    send[:, 80:96, :] = jnp.broadcast_to(extra[None], (PEERS, 16, LANE))
    gn = jnp.where(row < ROWS - 1, pltpu.roll(a, ROWS - 1, 0), 1.0)
    step = 1
    while step < ROWS:
        ok = row < ROWS - step
        gn = jnp.where(ok, gn * pltpu.roll(gn, ROWS - step, 0), gn)
        step *= 2
    gain[...] = gn


def states_body(sp_ref, got, a, cum, loc, logits, q, rr, s1, gv, lru, r_out, coef):
    sp = sp_ref[0]
    row = iota((PEERS, CH), 0)
    ends = got[:, 80:96, :].astype(F32)
    line = iota((PEERS, 16, LANE), 1)
    halves = [jnp.sum(jnp.where(line // 3 == k, ends, 0.0), axis=1) for k in range(4)]
    gn = jnp.concatenate(halves[:2], axis=1)
    terms = jnp.concatenate(halves[2:], axis=1)
    fwd = jnp.where(row < sp, gn, 1.0)
    fwd = jnp.where(row < PEERS - 1, pltpu.roll(fwd, PEERS - 1, 0), 1.0)
    rev = jnp.where(row > sp, gn, 1.0)
    rev = jnp.where(row > 0, pltpu.roll(rev, 1, 0), 1.0)
    step = 1
    while step < PEERS:
        fwd = jnp.where(row < PEERS - step, fwd * pltpu.roll(fwd, PEERS - step, 0), fwd)
        rev = jnp.where(row >= step, rev * pltpu.roll(rev, step, 0), rev)
        step *= 2
    carry = jnp.sum(jnp.where(row < sp, terms * fwd, 0.0), axis=0, keepdims=True)
    coef[...] = jnp.where(row > sp, rev, 0.0)
    st = loc[...] + cum[...] * carry
    wide = iota((ROWS, CH), 0)
    prev = jnp.where(wide > 0, pltpu.roll(st, 1, 0), carry)
    z = logits[...].astype(F32)
    k = 0.7978845608028654
    t = jnp.tanh(k * (z + 0.044715 * z * z * z))
    val = 0.5 * z * (1.0 + t)
    der = 0.5 * (1.0 + t) + 0.5 * z * (1.0 - t * t) * k * (1.0 + 3.0 * 0.044715 * z * z)
    s1[...] = st * der
    gv[...] = val
    lru[...] = (st * val).astype(BF)
    r_out[...] = rr[...] * (prev * a[...] - q[...])


def reverse_body(full, *refs):
    far, (gate_pre, tail_sum, out, send), rest = refs[:5], refs[5:9], refs[9:]
    (lru, wout, gv, a_ref, s1), (sem_in, sem) = rest[:5], rest[5:]
    arrivals = bring(list(zip(far, (lru, wout, gv, a_ref, s1))), sem_in)
    arrivals[0].wait()
    lv = lru[...]
    copies = []
    for t in range(TPN):
        part = mm(full[t], lv, 0, 0).astype(BF)
        send[8 * t : 8 * t + 8, 0:64, :] = part.reshape(8, 64, CH)
        rows = pl.ds(8 * t, 8), pl.ds(0, 64)
        copies.append(pltpu.make_async_copy(send.at[rows], out.at[rows], sem.at[t]))
        copies[t].start()
    arrivals[1].wait()
    mixer = mm(full[0], wout[0:512, :])
    for t in range(1, TPN):
        mixer = mixer + mm(full[t], wout[t * 512 : (t + 1) * 512, :])
    arrivals[2].wait()
    arrivals[3].wait()
    row = iota((ROWS, CH), 0)
    a = a_ref[...]
    gn = jnp.where(row < ROWS - 1, pltpu.roll(a, ROWS - 1, 0), 1.0)
    s = mixer * gv[...]
    step = 1
    while step < ROWS:
        ok = row < ROWS - step
        s = jnp.where(ok, s + gn * pltpu.roll(s, ROWS - step, 0), s)
        gn = jnp.where(ok, gn * pltpu.roll(gn, ROWS - step, 0), gn)
        step *= 2
    term = a[0:1] * s[0:1]
    pieces = jnp.concatenate(in_three(term) + [jnp.zeros((5, CH), F32)], axis=0).astype(BF)
    send[:, 64:72, :] = jnp.broadcast_to(pieces[None], (PEERS, 8, CH))
    rows = pl.ds(0, PEERS), pl.ds(64, 8)
    copies.append(pltpu.make_async_copy(send.at[rows], out.at[rows], sem.at[TPN]))
    copies[TPN].start()
    tail_sum[...] = s
    arrivals[4].wait()
    gate_pre[...] = mixer * s1[...]
    for copy in copies:
        copy.wait()


def final_body(got, coef, tail_sum, gain, rr, ad, scaled, wr, wi, out_proj, grad_in):
    acc = got[0, 0:64, :].astype(F32)
    for s in range(1, PEERS):
        acc = acc + got[s, 0:64, :].astype(F32)
    out_proj[...] = acc
    terms = jnp.sum(got[:, 64:72, :].astype(F32), axis=1)
    carry = jnp.sum(terms * coef[...], axis=0, keepdims=True)
    sg = tail_sum[...] + gain[...] * carry
    d_recall = (sg * rr[...]).astype(BF)
    d_admit = (sg * ad[...]).astype(BF)
    base = sg * scaled[...]
    for n in range(2):
        cols = slice(n * LANE, (n + 1) * LANE)
        back = mm(d_recall[:, cols], wr[n], 1, 1) + mm(d_admit[:, cols], wi[n], 1, 1)
        grad_in[:, cols] = base[:, cols] + back


RING = [(i, (i + 1) % TPN) for i in range(TPN)]
BACK = [(i, (i - 1) % TPN) for i in range(TPN)]


def move(value, where):
    return lax.ppermute(value, "tp", where)


def ring_parts_a(own):
    half = PEERS // 2
    low, high = own[:half], own[half:]
    left1 = move(low, RING)
    right2 = move(high, BACK)
    left2 = move(high, RING)
    right1 = move(low, BACK)
    far1 = move(left1, RING)
    far2 = move(right2, BACK)
    return own, left1, left2, right1, right2, far1, far2


def ring_parts_b(own):
    half = PEERS // 2
    rows = own[:, :80]
    left = move(rows, RING)
    right = move(rows, BACK)
    far1 = move(left[:half], RING)
    far2 = move(right[half:], BACK)
    return own, left, right, far1, far2


def shape(*dims, dtype=BF):
    return jax.ShapeDtypeStruct(dims, dtype)


def expert_chain(tail, tp, parts, weights):
    rows = PEERS * (10 if tail else 8)
    size = 40 if tail else 32
    out = [shape(rows, WIDTH), shape(rows, WIDTH)] + [shape(rows, HID)] * 3
    out.append(shape(PEERS, TPN * size, LANE))

    def body(*refs):
        chain_body(tail, *refs)

    flops = 10 * rows * WIDTH * HID
    held = [(TPN, PEERS, 80 if tail else 64, LANE)] + [o.shape for o in out]
    held += [(WIDTH, HID), (WIDTH, HID), (HID, WIDTH)]
    scratch = [pltpu.VMEM(dims, BF) for dims in held] + [dma(7), dma(6), dma(9)]
    *saved, partial_value = call(
        body,
        out,
        len(parts) + 4,
        flops,
        12 << 20,
        smem=(0,),
        far=range(1, len(parts) + 4),
        far_out=range(6),
        scratch=scratch,
    )(tp, *parts, *weights)
    return saved, partial_value.reshape(PEERS * TPN, size, LANE)


def per_device(
    middle_stream,
    output_gradient,
    routes,
    chosen_expert_weight,
    expert_gate_weight,
    expert_up_weight,
    expert_down_weight,
    recurrent_output_weight,
    recurrence_input,
    output_gate_logits,
    recurrence_gate_weight,
    input_gate_weight,
    channel_decay_param,
    extra_log_decay,
):
    tp = lax.axis_index("tp").reshape(1).astype(jnp.int32)
    sp = lax.axis_index("sp").reshape(1).astype(jnp.int32)
    weights = (expert_gate_weight[0], expert_up_weight[0], expert_down_weight[0])

    tokens = (chosen_expert_weight.T, middle_stream, output_gradient)
    send_a, idx = call(
        pack_body,
        [shape(PEERS, 64, LANE), shape(8, ROWS, dtype=jnp.int32)],
        4,
        1 << 30,
        3 << 20,
    )(routes.T, *tokens)
    own_a = lax.all_to_all(send_a, "sp", 0, 0, tiled=True)
    first = lax.axis_index("tp") * 2
    recall_weight = lax.dynamic_slice_in_dim(recurrence_gate_weight, first, 2, 0)
    admit_weight = lax.dynamic_slice_in_dim(input_gate_weight, first, 2, 0)
    u_blocks = recurrence_input.reshape(ROWS, 2, LANE)

    def gate(weight):
        return jax.nn.sigmoid(
            jnp.einsum("tnb,nbc->tnc", u_blocks, weight, preferred_element_type=F32).reshape(
                ROWS, CH
            )
        )

    recall, admit = gate(recall_weight), gate(admit_weight)
    rate = -8.0 * jax.nn.softplus(-channel_decay_param)[None, :]
    log_decay = rate * recall + extra_log_decay
    decay = jnp.exp(log_decay)
    scale = jnp.sqrt(-jnp.expm1(2.0 * log_decay))
    u = recurrence_input.astype(F32)
    scaled = admit * scale
    driven = u * scaled
    minus = u * admit * decay * decay / scale
    of_recall = rate * recall * (1.0 - recall)
    of_admit = driven * (1.0 - admit)
    tile = shape(ROWS, CH, dtype=F32)
    cum, loc, gain, send_b = call(
        scan_body, [tile, tile, tile, shape(PEERS, 96, LANE)], 6, 1 << 28, 2 << 20
    )(decay, driven, idx, *tokens)
    own_a, send_b = lax.optimization_barrier((own_a, send_b))
    own_b = lax.all_to_all(send_b, "sp", 0, 0, tiled=True)
    parts_a = ring_parts_a(own_a)
    parts_b = ring_parts_b(own_b)
    s1, gelu_val, lru, of_log, coef = call(
        states_body,
        [tile, tile, shape(ROWS, CH), tile, shape(PEERS, CH, dtype=F32)],
        8,
        1 << 28,
        2 << 20,
        smem=(0,),
    )(sp, own_b, decay, cum, loc, output_gate_logits, minus, of_recall)

    saved_a, part_a = expert_chain(False, tp, parts_a, weights)
    got_a = lax.all_to_all(part_a, ("sp", "tp"), 0, 0, tiled=True)
    saved_b, part_b = expert_chain(True, tp, parts_b, weights)
    got_b = lax.all_to_all(part_b, ("sp", "tp"), 0, 0, tiled=True)

    x, cot, hid, dg, du = (jnp.concatenate([a, b], axis=0) for a, b in zip(saved_a, saved_b))
    grad_down = mm(hid, cot, 0, 0).astype(BF)
    grad_gate = mm(x, dg, 0, 0).astype(BF)
    grad_up = mm(x, du, 0, 0).astype(BF)

    columns = idx.T
    (so_far,) = call(combine_a_body, [shape(ROWS, 512, dtype=F32)], 3, 1 << 30, 2 << 20, 12)(
        got_a, columns, output_gradient
    )
    (spread,) = call(
        combine_b_body,
        [shape(TPN, ROWS, 512)],
        3,
        1 << 30,
        3 << 20,
        12,
        far=(2,),
        far_out=(0,),
        scratch=[pltpu.VMEM((ROWS, 512), BF), pltpu.VMEM((ROWS, 512), F32), dma(1), dma(TPN)],
    )(got_b, columns, so_far)
    full = lax.all_to_all(spread, "tp", 0, 0, tiled=True)
    grad_gate_pre, tail_sum, send = call(
        reverse_body,
        [tile, tile, shape(PEERS, 72, CH)],
        6,
        1 << 30,
        4 << 20,
        12,
        far=range(1, 6),
        far_out=(2,),
        scratch=[
            pltpu.VMEM((PEERS, 72, CH), BF),
            pltpu.VMEM((ROWS, CH), BF),
            pltpu.VMEM((WIDTH, CH), BF),
            pltpu.VMEM((ROWS, CH), F32),
            pltpu.VMEM((ROWS, CH), F32),
            pltpu.VMEM((ROWS, CH), F32),
            dma(5),
            dma(TPN + 1),
        ],
    )(full, lru, recurrent_output_weight, gelu_val, decay, s1)
    got = lax.all_to_all(send, "sp", 0, 0, tiled=True)
    grad_out_proj, grad_input = call(
        final_body, [shape(64, CH, dtype=F32), tile], 9, 1 << 28, 3 << 20, 8
    )(got, coef, tail_sum, gain, of_log, of_admit, scaled, recall_weight, admit_weight)
    return (
        grad_gate[None],
        grad_up[None],
        grad_down[None],
        grad_out_proj,
        grad_input,
        grad_gate_pre,
    )


def solution(mesh):
    placed = (
        P("sp", "tp"),
        P("sp", "tp"),
        P("sp", None),
        P("sp", None),
        P("sp", None, "tp"),
        P("sp", None, "tp"),
        P("sp", "tp", None),
        P(None, "tp"),
        P("sp", "tp"),
        P("sp", "tp"),
        P(),
        P(),
        P("tp"),
        P("sp", "tp"),
    )

    return jax.shard_map(
        per_device,
        mesh=mesh,
        in_specs=placed,
        out_specs=(
            P("sp", None, "tp"),
            P("sp", None, "tp"),
            P("sp", "tp", None),
            P("sp", "tp"),
            P("sp", "tp"),
            P("sp", "tp"),
        ),
        check_vma=False,
    )
```

```python
import jax
import jax.numpy as jnp
from jax import lax
from jax.experimental import pallas as pl
from jax.experimental.pallas import tpu as pltpu
from jax.sharding import PartitionSpec as P

BF = jnp.bfloat16
F32 = jnp.float32
ROWS = 192
PEERS = 32
TPN = 4
LANE = 128
CH = 256
HID = 896
WIDTH = 2048
VMEM = pl.BlockSpec(memory_space=pltpu.VMEM)
SMEM = pl.BlockSpec(memory_space=pltpu.SMEM)
HBM = pl.BlockSpec(memory_space=pltpu.HBM)


def mm(a, b, ca=1, cb=0):
    return lax.dot_general(a, b, (((ca,), (cb,)), ((), ())), preferred_element_type=F32)


def iota(shape, dim):
    return lax.broadcasted_iota(jnp.int32, shape, dim)


def call(body, out, n_in, flops, moved, mib=56, smem=(), far=(), far_out=(), scratch=()):
    kinds = {**dict.fromkeys(smem, SMEM), **dict.fromkeys(far, HBM)}
    return pl.pallas_call(
        body,
        out_shape=out,
        in_specs=[kinds.get(k, VMEM) for k in range(n_in)],
        out_specs=[HBM if k in far_out else VMEM for k in range(len(out))],
        scratch_shapes=list(scratch),
        cost_estimate=pl.CostEstimate(flops=flops, bytes_accessed=moved, transcendentals=0),
        compiler_params=pltpu.CompilerParams(vmem_limit_bytes=mib * 1024 * 1024),
    )


def dma(count):
    return pltpu.SemaphoreType.DMA((count,))


def pack_main(block, out, base, pieces):
    rows = block.reshape(PEERS, 8, pieces * LANE)
    for pair in range(pieces // 2):
        lo = rows[:, :, 2 * pair * LANE : (2 * pair + 1) * LANE]
        hi = rows[:, :, (2 * pair + 1) * LANE : (2 * pair + 2) * LANE]
        at = base + pair * 16
        out[:, at : at + 16, :] = jnp.concatenate([lo, hi], axis=1).astype(BF)


def unpack_main(block, pair):
    got = block[:, pair * 16 : pair * 16 + 16, :].astype(F32)
    lo = got[:, :8, :].reshape(PEERS * 8, LANE).astype(BF)
    hi = got[:, 8:, :].reshape(PEERS * 8, LANE).astype(BF)
    return lo, hi


def tail_order(pieces):
    n = PEERS * pieces * 2
    r, c = iota((n, n), 0), iota((n, n), 1)
    peer, piece, slot = r // (pieces * 2), (r // 2) % pieces, r % 2
    return (piece * (PEERS * 2) + peer * 2 + slot == c).astype(F32).astype(BF)


def tail_order_back(pieces):
    n = PEERS * pieces * 2
    r, c = iota((n, n), 0), iota((n, n), 1)
    peer, piece, slot = c // (pieces * 2), (c // 2) % pieces, c % 2
    return (piece * (PEERS * 2) + peer * 2 + slot == r).astype(F32).astype(BF)


def weighted(weights, g):
    same = iota((ROWS, ROWS), 0) == iota((ROWS, ROWS), 1)
    gf = g[...].astype(F32)
    cots = []
    for k in range(2):
        w = jnp.sum(jnp.where(same, weights[k : k + 1, :], 0.0), axis=1, keepdims=True)
        cots.append((w * gf).astype(BF))
    return jnp.concatenate(cots, axis=0)


def chosen(at0, at1, n, x, both):
    r = iota((n, ROWS), 0)
    p0, p1 = (r == at0).astype(F32), (r == at1).astype(F32)
    return (
        mm((p0 + p1).astype(BF), x),
        mm(jnp.concatenate([p0, p1], axis=1).astype(BF), both),
    )


def pack_body(routes, weights, x, g, out_a, out_idx):
    experts = iota((PEERS, ROWS), 0)
    before = (iota((ROWS, ROWS), 0) < iota((ROWS, ROWS), 1)).astype(F32).astype(BF)
    r0, r1 = routes[0:1, :], routes[1:2, :]
    o0 = (experts == r0).astype(F32)
    o1 = (experts == r1).astype(F32)
    c0 = mm(o0.astype(BF), before)
    c1 = mm(o1.astype(BF), before) + jnp.sum(o0, axis=1, keepdims=True)
    k0 = jnp.sum(o0 * c0, axis=0, keepdims=True).astype(jnp.int32)
    k1 = jnp.sum(o1 * c1, axis=0, keepdims=True).astype(jnp.int32)
    idx = []
    for low, high in ((0, 8), (8, 16), (16, 18)):
        for r, k in ((r0, k0), (r1, k1)):
            here = (k >= low) & (k < high)
            idx.append(jnp.where(here, r * (high - low) + k - low, -1))
    none = jnp.full((1, ROWS), -1, jnp.int32)
    out_idx[...] = jnp.concatenate(idx + [none, none], axis=0)
    both = weighted(weights, g)
    xv = x[...]
    xm, cm = chosen(idx[0], idx[1], PEERS * 8, xv, both)
    pack_main(xm, out_a, 0, 4)
    pack_main(cm, out_a, 32, 4)


def chain_body(tail, tp_ref, *refs):
    parts, weights, outs, rest = refs[:7], refs[7:10], refs[10:16], refs[16:]
    values, x, c, hid, dg, du, out, wg, wu, wd, sem_in, sem_w, sem_out = rest
    main = PEERS * 8
    half = PEERS // 2
    depth = 80 if tail else 64
    size = 40 if tail else 32
    places = [values.at[0]] + [values.at[s, pl.ds(h * half, half)] for s in (1, 2, 3) for h in (0, 1)]
    arrivals = ((0,), (1, 2), (3, 4), (5, 6))
    fetch = [
        pltpu.make_async_copy(p.at[:, 0:depth] if k == 0 else p, place, sem_in.at[k])
        for k, (p, place) in enumerate(zip(parts, places))
    ]
    loads = []
    for k, (w, v) in enumerate(zip(weights, (wg, wu, wd))):
        n = w.shape[0] // 2
        loads += [
            pltpu.make_async_copy(w.at[pl.ds(h * n, n)], v.at[pl.ds(h * n, n)], sem_w.at[2 * k + h])
            for h in range(2)
        ]
    for copy in fetch + loads[:2]:
        copy.start()
    saves = [
        pltpu.make_async_copy(v, o, sem_out.at[k])
        for k, (v, o) in enumerate(zip((x, c, hid, dg, du), outs))
    ]
    saves += [
        pltpu.make_async_copy(
            out.at[:, t * size : (t + 1) * size], outs[5].at[:, t * size : (t + 1) * size], sem_out.at[5 + t]
        )
        for t in range(TPN)
    ]
    tp = tp_ref[0]

    def at(off):
        return pl.multiple_of(((tp + off) % TPN) * 512, 512)

    if tail:
        order = tail_order_back(8)
    for source, (off, arriving) in enumerate(zip((0, 3, 1, 2), arrivals)):
        for k in arriving:
            fetch[k].wait()
        if source == 3:
            for load in loads[2:]:
                load.start()
        value = values[source]
        for q2 in range(4):
            lo, hi = unpack_main(value, q2)
            dest = x if q2 < 2 else c
            col = at(off) + (q2 % 2) * 256
            dest[0:main, pl.ds(col, 256)] = jnp.concatenate([lo, hi], axis=1)
    if tail:
        lines = [values[source, :, 64:80, :].reshape(PEERS * 16, LANE) for source in range(TPN)]
        rows = mm(order, jnp.concatenate(lines, axis=1)).astype(BF)
        for source, off in enumerate((0, 3, 1, 2)):
            cols = slice(source * LANE, (source + 1) * LANE)
            for q in range(8):
                dest = x if q < 4 else c
                dest[main : main + 64, pl.ds(at(off) + (q % 4) * LANE, LANE)] = rows[
                    q * 64 : (q + 1) * 64, cols
                ]
    xv, cv = x[...], c[...]
    for load in loads[0:2]:
        load.wait()
    gate = mm(xv, wg[...])
    for load in loads[2:4]:
        load.wait()
    up = mm(xv, wu[...])
    for load in loads[4:6]:
        load.wait()
    dh = mm(cv, wd[...], 1, 1)
    saves[0].start()
    saves[1].start()
    sig = 1.0 / (1.0 + jnp.exp(-gate))
    silu = gate * sig
    hid[...] = (silu * up).astype(BF)
    dg[...] = (dh * up * sig * (1.0 + gate * (1.0 - sig))).astype(BF)
    du[...] = (dh * silu).astype(BF)
    for k in (2, 3, 4):
        saves[k].start()
    dgv, duv = dg[...], du[...]
    if tail:
        order = tail_order(4)
    for t in range(TPN):
        part = mm(dgv, wg[t * 512 : (t + 1) * 512, :], 1, 1)
        part = part + mm(duv, wu[t * 512 : (t + 1) * 512, :], 1, 1)
        pack_main(part[:main], out, t * size, 4)
        if tail:
            pieces = [part[main:, q * LANE : (q + 1) * LANE] for q in range(4)]
            put = mm(order, jnp.concatenate(pieces, axis=0).astype(BF))
            out[:, t * size + 32 : t * size + 40, :] = put.reshape(PEERS, 8, LANE).astype(BF)
        saves[5 + t].start()
    for save in saves:
        save.wait()


def slot_mask(idx, code, first):
    at0, at1 = idx[:, first : first + 1], idx[:, first + 1 : first + 2]
    return ((code == at0) | (code == at1)).astype(F32)


def add_main(got, idx, first):
    n = PEERS * TPN
    m = iota((1, n * 16), 1)
    both = slot_mask(idx, (m // 64) * 8 + m % 8, first)
    half = (m // 8) % 2
    values = [got[:, 16 * p : 16 * p + 16, :].reshape(n * 16, LANE) for p in range(2)]
    value = jnp.concatenate(values, axis=1)
    even, odd = [mm(jnp.where(half == k, both, 0.0).astype(BF), value) for k in range(2)]
    return [even[:, :LANE], odd[:, :LANE], even[:, LANE:], odd[:, LANE:]]


def combine_a_body(got, idx, g, out):
    out[...] = g[...].astype(F32) + jnp.concatenate(add_main(got, idx, 0), axis=1)


def bring(pairs, sem):
    copies = [pltpu.make_async_copy(src, dst, sem.at[k]) for k, (src, dst) in enumerate(pairs)]
    for copy in copies:
        copy.start()
    return copies


def combine_b_body(got, idx, so_far_far, out, res, so_far, sem_in, sem):
    (early,) = bring([(so_far_far, so_far)], sem_in)
    n = PEERS * TPN
    acc = add_main(got, idx, 2)
    m = iota((1, n * 8), 1)
    both = slot_mask(idx, (m // 32) * 2 + m % 2, 4)
    value = got[:, 32:40, :].reshape(n * 8, LANE)
    for q in range(4):
        acc[q] = acc[q] + mm(jnp.where((m // 2) % 4 == q, both, 0.0).astype(BF), value)
    early.wait()
    res[...] = (so_far[...] + jnp.concatenate(acc, axis=1)).astype(BF)
    copies = [pltpu.make_async_copy(res, out.at[t], sem.at[t]) for t in range(TPN)]
    for copy in copies:
        copy.start()
    for copy in copies:
        copy.wait()


def in_three(v):
    hi = v.astype(BF)
    rest = v - hi.astype(F32)
    mid = rest.astype(BF)
    low = (rest - mid.astype(F32)).astype(BF)
    return [p.astype(F32) for p in (hi, mid, low)]


def scan_body(a_ref, b_ref, idx, weights, x, g, cum, loc, gain, send):
    both = weighted(weights, g)
    xv = x[...]
    xm, cm = chosen(idx[2:3, :], idx[3:4, :], PEERS * 8, xv, both)
    pack_main(xm, send, 0, 4)
    pack_main(cm, send, 32, 4)
    xt, ct = chosen(idx[4:5, :], idx[5:6, :], PEERS * 2, xv, both)
    pieces = [v[:, q * LANE : (q + 1) * LANE] for v in (xt, ct) for q in range(4)]
    tail = mm(tail_order(8), jnp.concatenate(pieces, axis=0).astype(BF))
    send[:, 64:80, :] = tail.astype(BF).reshape(PEERS, 16, LANE)
    a = a_ref[...]
    row = iota((ROWS, CH), 0)
    ca, cb = a, b_ref[...]
    step = 1
    while step < ROWS:
        ok = row >= step
        pa, pb = pltpu.roll(ca, step, 0), pltpu.roll(cb, step, 0)
        cb = jnp.where(ok, ca * pb + cb, cb)
        ca = jnp.where(ok, ca * pa, ca)
        step *= 2
    cum[...] = ca
    loc[...] = cb
    lines = []
    for v in (ca[ROWS - 1 : ROWS], cb[ROWS - 1 : ROWS]):
        pieces = in_three(v)
        for h in range(2):
            lines += [p[:, h * LANE : (h + 1) * LANE] for p in pieces]
    lines.append(jnp.zeros((4, LANE), F32))
    extra = jnp.concatenate(lines, axis=0).astype(BF)
    send[:, 80:96, :] = jnp.broadcast_to(extra[None], (PEERS, 16, LANE))
    gn = jnp.where(row < ROWS - 1, pltpu.roll(a, ROWS - 1, 0), 1.0)
    step = 1
    while step < ROWS:
        ok = row < ROWS - step
        gn = jnp.where(ok, gn * pltpu.roll(gn, ROWS - step, 0), gn)
        step *= 2
    gain[...] = gn


def states_body(sp_ref, got, a, cum, loc, logits, q, rr, s1, gv, lru, r_out, coef):
    sp = sp_ref[0]
    row = iota((PEERS, CH), 0)
    ends = got[:, 80:96, :].astype(F32)
    line = iota((PEERS, 16, LANE), 1)
    halves = [jnp.sum(jnp.where(line // 3 == k, ends, 0.0), axis=1) for k in range(4)]
    gn = jnp.concatenate(halves[:2], axis=1)
    terms = jnp.concatenate(halves[2:], axis=1)
    fwd = jnp.where(row < sp, gn, 1.0)
    fwd = jnp.where(row < PEERS - 1, pltpu.roll(fwd, PEERS - 1, 0), 1.0)
    rev = jnp.where(row > sp, gn, 1.0)
    rev = jnp.where(row > 0, pltpu.roll(rev, 1, 0), 1.0)
    step = 1
    while step < PEERS:
        fwd = jnp.where(row < PEERS - step, fwd * pltpu.roll(fwd, PEERS - step, 0), fwd)
        rev = jnp.where(row >= step, rev * pltpu.roll(rev, step, 0), rev)
        step *= 2
    carry = jnp.sum(jnp.where(row < sp, terms * fwd, 0.0), axis=0, keepdims=True)
    coef[...] = jnp.where(row > sp, rev, 0.0)
    st = loc[...] + cum[...] * carry
    wide = iota((ROWS, CH), 0)
    prev = jnp.where(wide > 0, pltpu.roll(st, 1, 0), carry)
    z = logits[...].astype(F32)
    k = 0.7978845608028654
    t = jnp.tanh(k * (z + 0.044715 * z * z * z))
    val = 0.5 * z * (1.0 + t)
    der = 0.5 * (1.0 + t) + 0.5 * z * (1.0 - t * t) * k * (1.0 + 3.0 * 0.044715 * z * z)
    s1[...] = st * der
    gv[...] = val
    lru[...] = (st * val).astype(BF)
    r_out[...] = rr[...] * (prev * a[...] - q[...])


def reverse_body(full, *refs):
    far, (gate_pre, tail_sum, out, send), rest = refs[:5], refs[5:9], refs[9:]
    (lru, wout, gv, a_ref, s1), (sem_in, sem) = rest[:5], rest[5:]
    arrivals = bring(list(zip(far, (lru, wout, gv, a_ref, s1))), sem_in)
    arrivals[0].wait()
    lv = lru[...]
    copies = []
    for t in range(TPN):
        part = mm(full[t], lv, 0, 0).astype(BF)
        for h in range(2):
            piece = part[:, h * LANE : (h + 1) * LANE].reshape(8, 64, LANE)
            send[8 * t : 8 * t + 8, h * 64 : h * 64 + 64, :] = piece
        rows = pl.ds(8 * t, 8), pl.ds(0, 128)
        copies.append(pltpu.make_async_copy(send.at[rows], out.at[rows], sem.at[t]))
        copies[t].start()
    arrivals[1].wait()
    mixer = mm(full[0], wout[0:512, :])
    for t in range(1, TPN):
        mixer = mixer + mm(full[t], wout[t * 512 : (t + 1) * 512, :])
    arrivals[2].wait()
    arrivals[3].wait()
    row = iota((ROWS, CH), 0)
    a = a_ref[...]
    gn = jnp.where(row < ROWS - 1, pltpu.roll(a, ROWS - 1, 0), 1.0)
    s = mixer * gv[...]
    step = 1
    while step < ROWS:
        ok = row < ROWS - step
        s = jnp.where(ok, s + gn * pltpu.roll(s, ROWS - step, 0), s)
        gn = jnp.where(ok, gn * pltpu.roll(gn, ROWS - step, 0), gn)
        step *= 2
    term = a[0:1] * s[0:1]
    lines = [p[:, h * LANE : (h + 1) * LANE] for h in range(2) for p in in_three(term)]
    pieces = jnp.concatenate(lines + [jnp.zeros((2, LANE), F32)], axis=0).astype(BF)
    send[:, 128:136, :] = jnp.broadcast_to(pieces[None], (PEERS, 8, LANE))
    rows = pl.ds(0, PEERS), pl.ds(128, 8)
    copies.append(pltpu.make_async_copy(send.at[rows], out.at[rows], sem.at[TPN]))
    copies[TPN].start()
    tail_sum[...] = s
    arrivals[4].wait()
    gate_pre[...] = mixer * s1[...]
    for copy in copies:
        copy.wait()


def final_body(got, coef, tail_sum, gain, rr, ad, scaled, wr, wi, out_proj, grad_in):
    acc = got[0, 0:128, :].astype(F32)
    for s in range(1, PEERS):
        acc = acc + got[s, 0:128, :].astype(F32)
    out_proj[...] = jnp.concatenate([acc[0:64], acc[64:128]], axis=1)
    pieces = got[:, 128:136, :].astype(F32)
    line = iota((PEERS, 8, LANE), 1)
    halves = [jnp.sum(jnp.where(line // 3 == h, pieces, 0.0), axis=1) for h in range(2)]
    terms = jnp.concatenate(halves, axis=1)
    carry = jnp.sum(terms * coef[...], axis=0, keepdims=True)
    sg = tail_sum[...] + gain[...] * carry
    d_recall = (sg * rr[...]).astype(BF)
    d_admit = (sg * ad[...]).astype(BF)
    base = sg * scaled[...]
    for n in range(2):
        cols = slice(n * LANE, (n + 1) * LANE)
        back = mm(d_recall[:, cols], wr[n], 1, 1) + mm(d_admit[:, cols], wi[n], 1, 1)
        grad_in[:, cols] = base[:, cols] + back


RING = [(i, (i + 1) % TPN) for i in range(TPN)]
BACK = [(i, (i - 1) % TPN) for i in range(TPN)]


def move(value, where):
    return lax.ppermute(value, "tp", where)


def ring_parts(own, depth):
    half = PEERS // 2
    low, high = own[:half, :depth], own[half:, :depth]
    left1 = move(low, RING)
    right2 = move(high, BACK)
    left2 = move(high, RING)
    right1 = move(low, BACK)
    far1 = move(left1, RING)
    far2 = move(right2, BACK)
    return own, left1, left2, right1, right2, far1, far2


def shape(*dims, dtype=BF):
    return jax.ShapeDtypeStruct(dims, dtype)


def expert_chain(tail, tp, parts, weights):
    rows = PEERS * (10 if tail else 8)
    size = 40 if tail else 32
    out = [shape(rows, WIDTH), shape(rows, WIDTH)] + [shape(rows, HID)] * 3
    out.append(shape(PEERS, TPN * size, LANE))

    def body(*refs):
        chain_body(tail, *refs)

    flops = 10 * rows * WIDTH * HID
    held = [(TPN, PEERS, 80 if tail else 64, LANE)] + [o.shape for o in out]
    held += [(WIDTH, HID), (WIDTH, HID), (HID, WIDTH)]
    scratch = [pltpu.VMEM(dims, BF) for dims in held] + [dma(7), dma(6), dma(9)]
    *saved, partial_value = call(
        body,
        out,
        len(parts) + 4,
        flops,
        12 << 20,
        smem=(0,),
        far=range(1, len(parts) + 4),
        far_out=range(6),
        scratch=scratch,
    )(tp, *parts, *weights)
    return saved, partial_value.reshape(PEERS * TPN, size, LANE)


def per_device(
    middle_stream,
    output_gradient,
    routes,
    chosen_expert_weight,
    expert_gate_weight,
    expert_up_weight,
    expert_down_weight,
    recurrent_output_weight,
    recurrence_input,
    output_gate_logits,
    recurrence_gate_weight,
    input_gate_weight,
    channel_decay_param,
    extra_log_decay,
):
    tp = lax.axis_index("tp").reshape(1).astype(jnp.int32)
    sp = lax.axis_index("sp").reshape(1).astype(jnp.int32)
    weights = (expert_gate_weight[0], expert_up_weight[0], expert_down_weight[0])

    tokens = (chosen_expert_weight.T, middle_stream, output_gradient)
    send_a, idx = call(
        pack_body,
        [shape(PEERS, 64, LANE), shape(8, ROWS, dtype=jnp.int32)],
        4,
        1 << 30,
        3 << 20,
    )(routes.T, *tokens)
    own_a = lax.all_to_all(send_a, "sp", 0, 0, tiled=True)
    first = lax.axis_index("tp") * 2
    recall_weight = lax.dynamic_slice_in_dim(recurrence_gate_weight, first, 2, 0)
    admit_weight = lax.dynamic_slice_in_dim(input_gate_weight, first, 2, 0)
    u_blocks = recurrence_input.reshape(ROWS, 2, LANE)

    def gate(weight):
        return jax.nn.sigmoid(
            jnp.einsum("tnb,nbc->tnc", u_blocks, weight, preferred_element_type=F32).reshape(
                ROWS, CH
            )
        )

    recall, admit = gate(recall_weight), gate(admit_weight)
    rate = -8.0 * jax.nn.softplus(-channel_decay_param)[None, :]
    log_decay = rate * recall + extra_log_decay
    decay = jnp.exp(log_decay)
    scale = jnp.sqrt(-jnp.expm1(2.0 * log_decay))
    u = recurrence_input.astype(F32)
    scaled = admit * scale
    driven = u * scaled
    minus = u * admit * decay * decay / scale
    of_recall = rate * recall * (1.0 - recall)
    of_admit = driven * (1.0 - admit)
    tile = shape(ROWS, CH, dtype=F32)
    cum, loc, gain, send_b = call(
        scan_body, [tile, tile, tile, shape(PEERS, 96, LANE)], 6, 1 << 28, 2 << 20
    )(decay, driven, idx, *tokens)
    own_a, send_b = lax.optimization_barrier((own_a, send_b))
    own_b = lax.all_to_all(send_b, "sp", 0, 0, tiled=True)
    parts_a = ring_parts(own_a, 64)
    parts_b = ring_parts(own_b, 80)
    s1, gelu_val, lru, of_log, coef = call(
        states_body,
        [tile, tile, shape(ROWS, CH), tile, shape(PEERS, CH, dtype=F32)],
        8,
        1 << 28,
        2 << 20,
        smem=(0,),
    )(sp, own_b, decay, cum, loc, output_gate_logits, minus, of_recall)

    saved_a, part_a = expert_chain(False, tp, parts_a, weights)
    got_a = lax.all_to_all(part_a, ("sp", "tp"), 0, 0, tiled=True)
    saved_b, part_b = expert_chain(True, tp, parts_b, weights)
    got_b = lax.all_to_all(part_b, ("sp", "tp"), 0, 0, tiled=True)

    x, cot, hid, dg, du = (jnp.concatenate([a, b], axis=0) for a, b in zip(saved_a, saved_b))
    grad_down = mm(hid, cot, 0, 0).astype(BF)
    grad_gate = mm(x, dg, 0, 0).astype(BF)
    grad_up = mm(x, du, 0, 0).astype(BF)

    columns = idx.T
    (so_far,) = call(combine_a_body, [shape(ROWS, 512, dtype=F32)], 3, 1 << 30, 2 << 20, 12)(
        got_a, columns, output_gradient
    )
    (spread,) = call(
        combine_b_body,
        [shape(TPN, ROWS, 512)],
        3,
        1 << 30,
        3 << 20,
        12,
        far=(2,),
        far_out=(0,),
        scratch=[pltpu.VMEM((ROWS, 512), BF), pltpu.VMEM((ROWS, 512), F32), dma(1), dma(TPN)],
    )(got_b, columns, so_far)
    full = lax.all_to_all(spread, "tp", 0, 0, tiled=True)
    grad_gate_pre, tail_sum, send = call(
        reverse_body,
        [tile, tile, shape(PEERS, 136, LANE)],
        6,
        1 << 30,
        4 << 20,
        12,
        far=range(1, 6),
        far_out=(2,),
        scratch=[
            pltpu.VMEM((PEERS, 136, LANE), BF),
            pltpu.VMEM((ROWS, CH), BF),
            pltpu.VMEM((WIDTH, CH), BF),
            pltpu.VMEM((ROWS, CH), F32),
            pltpu.VMEM((ROWS, CH), F32),
            pltpu.VMEM((ROWS, CH), F32),
            dma(5),
            dma(TPN + 1),
        ],
    )(full, lru, recurrent_output_weight, gelu_val, decay, s1)
    got = lax.all_to_all(send, "sp", 0, 0, tiled=True)
    grad_out_proj, grad_input = call(
        final_body, [shape(64, CH, dtype=F32), tile], 9, 1 << 28, 3 << 20, 8
    )(got, coef, tail_sum, gain, of_log, of_admit, scaled, recall_weight, admit_weight)
    return (
        grad_gate[None],
        grad_up[None],
        grad_down[None],
        grad_out_proj,
        grad_input,
        grad_gate_pre,
    )


def solution(mesh):
    placed = (
        P("sp", "tp"),
        P("sp", "tp"),
        P("sp", None),
        P("sp", None),
        P("sp", None, "tp"),
        P("sp", None, "tp"),
        P("sp", "tp", None),
        P(None, "tp"),
        P("sp", "tp"),
        P("sp", "tp"),
        P(),
        P(),
        P("tp"),
        P("sp", "tp"),
    )

    return jax.shard_map(
        per_device,
        mesh=mesh,
        in_specs=placed,
        out_specs=(
            P("sp", None, "tp"),
            P("sp", None, "tp"),
            P("sp", "tp", None),
            P("sp", "tp"),
            P("sp", "tp"),
            P("sp", "tp"),
        ),
        check_vma=False,
    )
```

```python
import jax
import jax.numpy as jnp
from jax import lax
from jax.experimental import pallas as pl
from jax.experimental.pallas import tpu as pltpu
from jax.sharding import PartitionSpec as P

BF = jnp.bfloat16
F32 = jnp.float32
ROWS = 192
PEERS = 32
TPN = 4
LANE = 128
CH = 256
HID = 896
WIDTH = 2048
VMEM = pl.BlockSpec(memory_space=pltpu.VMEM)
SMEM = pl.BlockSpec(memory_space=pltpu.SMEM)
HBM = pl.BlockSpec(memory_space=pltpu.HBM)


def mm(a, b, ca=1, cb=0):
    return lax.dot_general(a, b, (((ca,), (cb,)), ((), ())), preferred_element_type=F32)


def iota(shape, dim):
    return lax.broadcasted_iota(jnp.int32, shape, dim)


def call(body, out, n_in, flops, moved, mib=56, smem=(), far=(), far_out=(), scratch=()):
    kinds = {**dict.fromkeys(smem, SMEM), **dict.fromkeys(far, HBM)}
    return pl.pallas_call(
        body,
        out_shape=out,
        in_specs=[kinds.get(k, VMEM) for k in range(n_in)],
        out_specs=[HBM if k in far_out else VMEM for k in range(len(out))],
        scratch_shapes=list(scratch),
        cost_estimate=pl.CostEstimate(flops=flops, bytes_accessed=moved, transcendentals=0),
        compiler_params=pltpu.CompilerParams(vmem_limit_bytes=mib * 1024 * 1024),
    )


def dma(count):
    return pltpu.SemaphoreType.DMA((count,))


def pack_main(block, out, base, pieces):
    rows = block.reshape(PEERS, 8, pieces * LANE)
    for pair in range(pieces // 2):
        lo = rows[:, :, 2 * pair * LANE : (2 * pair + 1) * LANE]
        hi = rows[:, :, (2 * pair + 1) * LANE : (2 * pair + 2) * LANE]
        at = base + pair * 16
        out[:, at : at + 16, :] = jnp.concatenate([lo, hi], axis=1).astype(BF)


def unpack_main(block, pair):
    got = block[:, pair * 16 : pair * 16 + 16, :].astype(F32)
    lo = got[:, :8, :].reshape(PEERS * 8, LANE).astype(BF)
    hi = got[:, 8:, :].reshape(PEERS * 8, LANE).astype(BF)
    return lo, hi


def tail_order(pieces):
    n = PEERS * pieces * 2
    r, c = iota((n, n), 0), iota((n, n), 1)
    peer, piece, slot = r // (pieces * 2), (r // 2) % pieces, r % 2
    return (piece * (PEERS * 2) + peer * 2 + slot == c).astype(F32).astype(BF)


def tail_order_back(pieces):
    n = PEERS * pieces * 2
    r, c = iota((n, n), 0), iota((n, n), 1)
    peer, piece, slot = c // (pieces * 2), (c // 2) % pieces, c % 2
    return (piece * (PEERS * 2) + peer * 2 + slot == r).astype(F32).astype(BF)


def weighted(weights, g):
    same = iota((ROWS, ROWS), 0) == iota((ROWS, ROWS), 1)
    gf = g[...].astype(F32)
    cots = []
    for k in range(2):
        w = jnp.sum(jnp.where(same, weights[k : k + 1, :], 0.0), axis=1, keepdims=True)
        cots.append((w * gf).astype(BF))
    return jnp.concatenate(cots, axis=0)


def chosen(at0, at1, n, x, both):
    r = iota((n, ROWS), 0)
    p0, p1 = (r == at0).astype(F32), (r == at1).astype(F32)
    return (
        mm((p0 + p1).astype(BF), x),
        mm(jnp.concatenate([p0, p1], axis=1).astype(BF), both),
    )


def pack_body(routes, weights, x, g, out_a, out_idx):
    experts = iota((PEERS, ROWS), 0)
    before = (iota((ROWS, ROWS), 0) < iota((ROWS, ROWS), 1)).astype(F32).astype(BF)
    r0, r1 = routes[0:1, :], routes[1:2, :]
    o0 = (experts == r0).astype(F32)
    o1 = (experts == r1).astype(F32)
    c0 = mm(o0.astype(BF), before)
    c1 = mm(o1.astype(BF), before) + jnp.sum(o0, axis=1, keepdims=True)
    k0 = jnp.sum(o0 * c0, axis=0, keepdims=True).astype(jnp.int32)
    k1 = jnp.sum(o1 * c1, axis=0, keepdims=True).astype(jnp.int32)
    idx = []
    for low, high in ((0, 8), (8, 16), (16, 18)):
        for r, k in ((r0, k0), (r1, k1)):
            here = (k >= low) & (k < high)
            idx.append(jnp.where(here, r * (high - low) + k - low, -1))
    none = jnp.full((1, ROWS), -1, jnp.int32)
    out_idx[...] = jnp.concatenate(idx + [none, none], axis=0)
    both = weighted(weights, g)
    xv = x[...]
    xm, cm = chosen(idx[0], idx[1], PEERS * 8, xv, both)
    pack_main(xm, out_a, 0, 4)
    pack_main(cm, out_a, 32, 4)


def chain_body(tail, tp_ref, *refs):
    parts, weights, outs, rest = refs[:7], refs[7:10], refs[10:16], refs[16:]
    values, x, c, hid, dg, du, out, wg, wu, wd, sem_in, sem_w, sem_out = rest
    main = PEERS * 8
    half = PEERS // 2
    depth = 80 if tail else 64
    size = 40 if tail else 32
    places = [values.at[0]] + [values.at[s, pl.ds(h * half, half)] for s in (1, 2, 3) for h in (0, 1)]
    arrivals = ((0,), (1, 2), (3, 4), (5, 6))
    fetch = [
        pltpu.make_async_copy(p.at[:, 0:depth] if k == 0 else p, place, sem_in.at[k])
        for k, (p, place) in enumerate(zip(parts, places))
    ]
    loads = []
    for k, (w, v) in enumerate(zip(weights, (wg, wu, wd))):
        n = w.shape[0] // 2
        loads += [
            pltpu.make_async_copy(w.at[pl.ds(h * n, n)], v.at[pl.ds(h * n, n)], sem_w.at[2 * k + h])
            for h in range(2)
        ]
    for copy in fetch:
        copy.start()
    saves = [
        pltpu.make_async_copy(v, o, sem_out.at[k])
        for k, (v, o) in enumerate(zip((x, c, hid, dg, du), outs))
    ]
    saves += [
        pltpu.make_async_copy(
            out.at[:, t * size : (t + 1) * size], outs[5].at[:, t * size : (t + 1) * size], sem_out.at[5 + t]
        )
        for t in range(TPN)
    ]
    tp = tp_ref[0]

    def at(off):
        return pl.multiple_of(((tp + off) % TPN) * 512, 512)

    if tail:
        order = tail_order_back(8)
    for source, (off, arriving) in enumerate(zip((0, 3, 1, 2), arrivals)):
        for k in arriving:
            fetch[k].wait()
        if source == 1:
            for load in loads[:2]:
                load.start()
        if source == 3:
            for load in loads[2:]:
                load.start()
        value = values[source]
        for q2 in range(4):
            lo, hi = unpack_main(value, q2)
            dest = x if q2 < 2 else c
            col = at(off) + (q2 % 2) * 256
            dest[0:main, pl.ds(col, 256)] = jnp.concatenate([lo, hi], axis=1)
    if tail:
        lines = [values[source, :, 64:80, :].reshape(PEERS * 16, LANE) for source in range(TPN)]
        rows = mm(order, jnp.concatenate(lines, axis=1)).astype(BF)
        for source, off in enumerate((0, 3, 1, 2)):
            cols = slice(source * LANE, (source + 1) * LANE)
            for q in range(8):
                dest = x if q < 4 else c
                dest[main : main + 64, pl.ds(at(off) + (q % 4) * LANE, LANE)] = rows[
                    q * 64 : (q + 1) * 64, cols
                ]
    xv, cv = x[...], c[...]
    for load in loads[0:2]:
        load.wait()
    gate = mm(xv, wg[...])
    for load in loads[2:4]:
        load.wait()
    up = mm(xv, wu[...])
    for load in loads[4:6]:
        load.wait()
    dh = mm(cv, wd[...], 1, 1)
    saves[0].start()
    saves[1].start()
    sig = 1.0 / (1.0 + jnp.exp(-gate))
    silu = gate * sig
    hid[...] = (silu * up).astype(BF)
    dg[...] = (dh * up * sig * (1.0 + gate * (1.0 - sig))).astype(BF)
    du[...] = (dh * silu).astype(BF)
    for k in (2, 3, 4):
        saves[k].start()
    dgv, duv = dg[...], du[...]
    if tail:
        order = tail_order(4)
    for t in range(TPN):
        part = mm(dgv, wg[t * 512 : (t + 1) * 512, :], 1, 1)
        part = part + mm(duv, wu[t * 512 : (t + 1) * 512, :], 1, 1)
        pack_main(part[:main], out, t * size, 4)
        if tail:
            pieces = [part[main:, q * LANE : (q + 1) * LANE] for q in range(4)]
            put = mm(order, jnp.concatenate(pieces, axis=0).astype(BF))
            out[:, t * size + 32 : t * size + 40, :] = put.reshape(PEERS, 8, LANE).astype(BF)
        saves[5 + t].start()
    for save in saves:
        save.wait()


def slot_mask(idx, code, first):
    at0, at1 = idx[:, first : first + 1], idx[:, first + 1 : first + 2]
    return ((code == at0) | (code == at1)).astype(F32)


def add_main(got, idx, first):
    n = PEERS * TPN
    m = iota((1, n * 16), 1)
    both = slot_mask(idx, (m // 64) * 8 + m % 8, first)
    half = (m // 8) % 2
    values = [got[:, 16 * p : 16 * p + 16, :].reshape(n * 16, LANE) for p in range(2)]
    value = jnp.concatenate(values, axis=1)
    even, odd = [mm(jnp.where(half == k, both, 0.0).astype(BF), value) for k in range(2)]
    return [even[:, :LANE], odd[:, :LANE], even[:, LANE:], odd[:, LANE:]]


def combine_a_body(got, idx, g, out):
    out[...] = g[...].astype(F32) + jnp.concatenate(add_main(got, idx, 0), axis=1)


def bring(pairs, sem):
    copies = [pltpu.make_async_copy(src, dst, sem.at[k]) for k, (src, dst) in enumerate(pairs)]
    for copy in copies:
        copy.start()
    return copies


def combine_b_body(got, idx, so_far_far, out, res, so_far, sem_in, sem):
    (early,) = bring([(so_far_far, so_far)], sem_in)
    n = PEERS * TPN
    acc = add_main(got, idx, 2)
    m = iota((1, n * 8), 1)
    both = slot_mask(idx, (m // 32) * 2 + m % 2, 4)
    value = got[:, 32:40, :].reshape(n * 8, LANE)
    for q in range(4):
        acc[q] = acc[q] + mm(jnp.where((m // 2) % 4 == q, both, 0.0).astype(BF), value)
    early.wait()
    res[...] = (so_far[...] + jnp.concatenate(acc, axis=1)).astype(BF)
    copies = [pltpu.make_async_copy(res, out.at[t], sem.at[t]) for t in range(TPN)]
    for copy in copies:
        copy.start()
    for copy in copies:
        copy.wait()


def in_three(v):
    hi = v.astype(BF)
    rest = v - hi.astype(F32)
    mid = rest.astype(BF)
    low = (rest - mid.astype(F32)).astype(BF)
    return [p.astype(F32) for p in (hi, mid, low)]


def scan_body(a_ref, b_ref, idx, weights, x, g, cum, loc, gain, send):
    both = weighted(weights, g)
    xv = x[...]
    xm, cm = chosen(idx[2:3, :], idx[3:4, :], PEERS * 8, xv, both)
    pack_main(xm, send, 0, 4)
    pack_main(cm, send, 32, 4)
    xt, ct = chosen(idx[4:5, :], idx[5:6, :], PEERS * 2, xv, both)
    pieces = [v[:, q * LANE : (q + 1) * LANE] for v in (xt, ct) for q in range(4)]
    tail = mm(tail_order(8), jnp.concatenate(pieces, axis=0).astype(BF))
    send[:, 64:80, :] = tail.astype(BF).reshape(PEERS, 16, LANE)
    a = a_ref[...]
    row = iota((ROWS, CH), 0)
    ca, cb = a, b_ref[...]
    step = 1
    while step < ROWS:
        ok = row >= step
        pa, pb = pltpu.roll(ca, step, 0), pltpu.roll(cb, step, 0)
        cb = jnp.where(ok, ca * pb + cb, cb)
        ca = jnp.where(ok, ca * pa, ca)
        step *= 2
    cum[...] = ca
    loc[...] = cb
    lines = []
    for v in (ca[ROWS - 1 : ROWS], cb[ROWS - 1 : ROWS]):
        pieces = in_three(v)
        for h in range(2):
            lines += [p[:, h * LANE : (h + 1) * LANE] for p in pieces]
    lines.append(jnp.zeros((4, LANE), F32))
    extra = jnp.concatenate(lines, axis=0).astype(BF)
    send[:, 80:96, :] = jnp.broadcast_to(extra[None], (PEERS, 16, LANE))
    gn = jnp.where(row < ROWS - 1, pltpu.roll(a, ROWS - 1, 0), 1.0)
    step = 1
    while step < ROWS:
        ok = row < ROWS - step
        gn = jnp.where(ok, gn * pltpu.roll(gn, ROWS - step, 0), gn)
        step *= 2
    gain[...] = gn


def states_body(sp_ref, got, a, cum, loc, logits, q, rr, s1, gv, lru, r_out, coef):
    sp = sp_ref[0]
    row = iota((PEERS, CH), 0)
    ends = got[:, 80:96, :].astype(F32)
    line = iota((PEERS, 16, LANE), 1)
    halves = [jnp.sum(jnp.where(line // 3 == k, ends, 0.0), axis=1) for k in range(4)]
    gn = jnp.concatenate(halves[:2], axis=1)
    terms = jnp.concatenate(halves[2:], axis=1)
    fwd = jnp.where(row < sp, gn, 1.0)
    fwd = jnp.where(row < PEERS - 1, pltpu.roll(fwd, PEERS - 1, 0), 1.0)
    rev = jnp.where(row > sp, gn, 1.0)
    rev = jnp.where(row > 0, pltpu.roll(rev, 1, 0), 1.0)
    step = 1
    while step < PEERS:
        fwd = jnp.where(row < PEERS - step, fwd * pltpu.roll(fwd, PEERS - step, 0), fwd)
        rev = jnp.where(row >= step, rev * pltpu.roll(rev, step, 0), rev)
        step *= 2
    carry = jnp.sum(jnp.where(row < sp, terms * fwd, 0.0), axis=0, keepdims=True)
    coef[...] = jnp.where(row > sp, rev, 0.0)
    st = loc[...] + cum[...] * carry
    wide = iota((ROWS, CH), 0)
    prev = jnp.where(wide > 0, pltpu.roll(st, 1, 0), carry)
    z = logits[...].astype(F32)
    k = 0.7978845608028654
    t = jnp.tanh(k * (z + 0.044715 * z * z * z))
    val = 0.5 * z * (1.0 + t)
    der = 0.5 * (1.0 + t) + 0.5 * z * (1.0 - t * t) * k * (1.0 + 3.0 * 0.044715 * z * z)
    s1[...] = st * der
    gv[...] = val
    lru[...] = (st * val).astype(BF)
    r_out[...] = rr[...] * (prev * a[...] - q[...])


def reverse_body(full, *refs):
    far, (gate_pre, tail_sum, out, send), rest = refs[:5], refs[5:9], refs[9:]
    (lru, wout, gv, a_ref, s1), (sem_in, sem) = rest[:5], rest[5:]
    arrivals = bring(list(zip(far, (lru, wout, gv, a_ref, s1))), sem_in)
    arrivals[0].wait()
    lv = lru[...]
    copies = []
    for t in range(TPN):
        part = mm(full[t], lv, 0, 0).astype(BF)
        for h in range(2):
            piece = part[:, h * LANE : (h + 1) * LANE].reshape(8, 64, LANE)
            send[8 * t : 8 * t + 8, h * 64 : h * 64 + 64, :] = piece
        rows = pl.ds(8 * t, 8), pl.ds(0, 128)
        copies.append(pltpu.make_async_copy(send.at[rows], out.at[rows], sem.at[t]))
        copies[t].start()
    arrivals[1].wait()
    mixer = mm(full[0], wout[0:512, :])
    for t in range(1, TPN):
        mixer = mixer + mm(full[t], wout[t * 512 : (t + 1) * 512, :])
    arrivals[2].wait()
    arrivals[3].wait()
    row = iota((ROWS, CH), 0)
    a = a_ref[...]
    gn = jnp.where(row < ROWS - 1, pltpu.roll(a, ROWS - 1, 0), 1.0)
    s = mixer * gv[...]
    step = 1
    while step < ROWS:
        ok = row < ROWS - step
        s = jnp.where(ok, s + gn * pltpu.roll(s, ROWS - step, 0), s)
        gn = jnp.where(ok, gn * pltpu.roll(gn, ROWS - step, 0), gn)
        step *= 2
    term = a[0:1] * s[0:1]
    lines = [p[:, h * LANE : (h + 1) * LANE] for h in range(2) for p in in_three(term)]
    pieces = jnp.concatenate(lines + [jnp.zeros((2, LANE), F32)], axis=0).astype(BF)
    send[:, 128:136, :] = jnp.broadcast_to(pieces[None], (PEERS, 8, LANE))
    rows = pl.ds(0, PEERS), pl.ds(128, 8)
    copies.append(pltpu.make_async_copy(send.at[rows], out.at[rows], sem.at[TPN]))
    copies[TPN].start()
    tail_sum[...] = s
    arrivals[4].wait()
    gate_pre[...] = mixer * s1[...]
    for copy in copies:
        copy.wait()


def final_body(got, coef, tail_sum, gain, rr, ad, scaled, wr, wi, out_proj, grad_in):
    acc = got[0, 0:128, :].astype(F32)
    for s in range(1, PEERS):
        acc = acc + got[s, 0:128, :].astype(F32)
    out_proj[...] = jnp.concatenate([acc[0:64], acc[64:128]], axis=1)
    pieces = got[:, 128:136, :].astype(F32)
    line = iota((PEERS, 8, LANE), 1)
    halves = [jnp.sum(jnp.where(line // 3 == h, pieces, 0.0), axis=1) for h in range(2)]
    terms = jnp.concatenate(halves, axis=1)
    carry = jnp.sum(terms * coef[...], axis=0, keepdims=True)
    sg = tail_sum[...] + gain[...] * carry
    d_recall = (sg * rr[...]).astype(BF)
    d_admit = (sg * ad[...]).astype(BF)
    base = sg * scaled[...]
    for n in range(2):
        cols = slice(n * LANE, (n + 1) * LANE)
        back = mm(d_recall[:, cols], wr[n], 1, 1) + mm(d_admit[:, cols], wi[n], 1, 1)
        grad_in[:, cols] = base[:, cols] + back


RING = [(i, (i + 1) % TPN) for i in range(TPN)]
BACK = [(i, (i - 1) % TPN) for i in range(TPN)]


def move(value, where):
    return lax.ppermute(value, "tp", where)


def ring_parts(own, depth):
    half = PEERS // 2
    low, high = own[:half, :depth], own[half:, :depth]
    left1 = move(low, RING)
    right2 = move(high, BACK)
    left2 = move(high, RING)
    right1 = move(low, BACK)
    far1 = move(left1, RING)
    far2 = move(right2, BACK)
    return own, left1, left2, right1, right2, far1, far2


def shape(*dims, dtype=BF):
    return jax.ShapeDtypeStruct(dims, dtype)


def expert_chain(tail, tp, parts, weights):
    rows = PEERS * (10 if tail else 8)
    size = 40 if tail else 32
    out = [shape(rows, WIDTH), shape(rows, WIDTH)] + [shape(rows, HID)] * 3
    out.append(shape(PEERS, TPN * size, LANE))

    def body(*refs):
        chain_body(tail, *refs)

    flops = 10 * rows * WIDTH * HID
    held = [(TPN, PEERS, 80 if tail else 64, LANE)] + [o.shape for o in out]
    held += [(WIDTH, HID), (WIDTH, HID), (HID, WIDTH)]
    scratch = [pltpu.VMEM(dims, BF) for dims in held] + [dma(7), dma(6), dma(9)]
    *saved, partial_value = call(
        body,
        out,
        len(parts) + 4,
        flops,
        12 << 20,
        smem=(0,),
        far=range(1, len(parts) + 4),
        far_out=range(6),
        scratch=scratch,
    )(tp, *parts, *weights)
    return saved, partial_value.reshape(PEERS * TPN, size, LANE)


def per_device(
    middle_stream,
    output_gradient,
    routes,
    chosen_expert_weight,
    expert_gate_weight,
    expert_up_weight,
    expert_down_weight,
    recurrent_output_weight,
    recurrence_input,
    output_gate_logits,
    recurrence_gate_weight,
    input_gate_weight,
    channel_decay_param,
    extra_log_decay,
):
    tp = lax.axis_index("tp").reshape(1).astype(jnp.int32)
    sp = lax.axis_index("sp").reshape(1).astype(jnp.int32)
    weights = (expert_gate_weight[0], expert_up_weight[0], expert_down_weight[0])

    tokens = (chosen_expert_weight.T, middle_stream, output_gradient)
    send_a, idx = call(
        pack_body,
        [shape(PEERS, 64, LANE), shape(8, ROWS, dtype=jnp.int32)],
        4,
        1 << 30,
        3 << 20,
    )(routes.T, *tokens)
    own_a = lax.all_to_all(send_a, "sp", 0, 0, tiled=True)
    first = lax.axis_index("tp") * 2
    recall_weight = lax.dynamic_slice_in_dim(recurrence_gate_weight, first, 2, 0)
    admit_weight = lax.dynamic_slice_in_dim(input_gate_weight, first, 2, 0)
    u_blocks = recurrence_input.reshape(ROWS, 2, LANE)

    def gate(weight):
        return jax.nn.sigmoid(
            jnp.einsum("tnb,nbc->tnc", u_blocks, weight, preferred_element_type=F32).reshape(
                ROWS, CH
            )
        )

    recall, admit = gate(recall_weight), gate(admit_weight)
    rate = -8.0 * jax.nn.softplus(-channel_decay_param)[None, :]
    log_decay = rate * recall + extra_log_decay
    decay = jnp.exp(log_decay)
    scale = jnp.sqrt(-jnp.expm1(2.0 * log_decay))
    u = recurrence_input.astype(F32)
    scaled = admit * scale
    driven = u * scaled
    minus = u * admit * decay * decay / scale
    of_recall = rate * recall * (1.0 - recall)
    of_admit = driven * (1.0 - admit)
    tile = shape(ROWS, CH, dtype=F32)
    cum, loc, gain, send_b = call(
        scan_body, [tile, tile, tile, shape(PEERS, 96, LANE)], 6, 1 << 28, 2 << 20
    )(decay, driven, idx, *tokens)
    own_a, send_b = lax.optimization_barrier((own_a, send_b))
    own_b = lax.all_to_all(send_b, "sp", 0, 0, tiled=True)
    parts_a = ring_parts(own_a, 64)
    parts_b = ring_parts(own_b, 80)
    s1, gelu_val, lru, of_log, coef = call(
        states_body,
        [tile, tile, shape(ROWS, CH), tile, shape(PEERS, CH, dtype=F32)],
        8,
        1 << 28,
        2 << 20,
        smem=(0,),
    )(sp, own_b, decay, cum, loc, output_gate_logits, minus, of_recall)

    saved_a, part_a = expert_chain(False, tp, parts_a, weights)
    got_a = lax.all_to_all(part_a, ("sp", "tp"), 0, 0, tiled=True)
    saved_b, part_b = expert_chain(True, tp, parts_b, weights)
    got_b = lax.all_to_all(part_b, ("sp", "tp"), 0, 0, tiled=True)

    x, cot, hid, dg, du = (jnp.concatenate([a, b], axis=0) for a, b in zip(saved_a, saved_b))
    grad_down = mm(hid, cot, 0, 0).astype(BF)
    grad_gate = mm(x, dg, 0, 0).astype(BF)
    grad_up = mm(x, du, 0, 0).astype(BF)

    columns = idx.T
    (so_far,) = call(combine_a_body, [shape(ROWS, 512, dtype=F32)], 3, 1 << 30, 2 << 20, 12)(
        got_a, columns, output_gradient
    )
    (spread,) = call(
        combine_b_body,
        [shape(TPN, ROWS, 512)],
        3,
        1 << 30,
        3 << 20,
        12,
        far=(2,),
        far_out=(0,),
        scratch=[pltpu.VMEM((ROWS, 512), BF), pltpu.VMEM((ROWS, 512), F32), dma(1), dma(TPN)],
    )(got_b, columns, so_far)
    full = lax.all_to_all(spread, "tp", 0, 0, tiled=True)
    grad_gate_pre, tail_sum, send = call(
        reverse_body,
        [tile, tile, shape(PEERS, 136, LANE)],
        6,
        1 << 30,
        4 << 20,
        12,
        far=range(1, 6),
        far_out=(2,),
        scratch=[
            pltpu.VMEM((PEERS, 136, LANE), BF),
            pltpu.VMEM((ROWS, CH), BF),
            pltpu.VMEM((WIDTH, CH), BF),
            pltpu.VMEM((ROWS, CH), F32),
            pltpu.VMEM((ROWS, CH), F32),
            pltpu.VMEM((ROWS, CH), F32),
            dma(5),
            dma(TPN + 1),
        ],
    )(full, lru, recurrent_output_weight, gelu_val, decay, s1)
    got = lax.all_to_all(send, "sp", 0, 0, tiled=True)
    grad_out_proj, grad_input = call(
        final_body, [shape(64, CH, dtype=F32), tile], 9, 1 << 28, 3 << 20, 8
    )(got, coef, tail_sum, gain, of_log, of_admit, scaled, recall_weight, admit_weight)
    return (
        grad_gate[None],
        grad_up[None],
        grad_down[None],
        grad_out_proj,
        grad_input,
        grad_gate_pre,
    )


def solution(mesh):
    placed = (
        P("sp", "tp"),
        P("sp", "tp"),
        P("sp", None),
        P("sp", None),
        P("sp", None, "tp"),
        P("sp", None, "tp"),
        P("sp", "tp", None),
        P(None, "tp"),
        P("sp", "tp"),
        P("sp", "tp"),
        P(),
        P(),
        P("tp"),
        P("sp", "tp"),
    )

    return jax.shard_map(
        per_device,
        mesh=mesh,
        in_specs=placed,
        out_specs=(
            P("sp", None, "tp"),
            P("sp", None, "tp"),
            P("sp", "tp", None),
            P("sp", "tp"),
            P("sp", "tp"),
            P("sp", "tp"),
        ),
        check_vma=False,
    )
```
